512 devices in a mesh: sp: 16 (over z), tp: 4 (over y), dp: 8 (over x, core).
Axes of the slice: x: 4, y: 4, z: 16, core: 2. Of those that a mesh axis runs over, the one named last changes fastest.
Arguments:
- latent: bfloat16 [8, 4096, 2048], P('dp', 'sp'), may hold values from -6 to 6
- context: bfloat16 [8, 512, 2048], P('dp', 'sp'), may hold values from -6 to 6
- condition: bfloat16 [8, 2048], P('dp'), may hold values from -6 to 6
- mod_weight: bfloat16 [2048, 6144], P(None, ('sp', 'tp')), may hold values from -0.125 to 0.125
- norm_gain: float32 [2048], replicated, may hold values from 0.1 to 1.9
- w_query: bfloat16 [2048, 1024], P(None, 'tp'), may hold values from -0.125 to 0.125
- w_key: bfloat16 [2048, 256], P(None, 'tp'), may hold values from -0.125 to 0.125
- w_value: bfloat16 [2048, 256], P(None, 'tp'), may hold values from -0.125 to 0.125
- q_gain: float32 [64], replicated, may hold values from 0.4 to 14, as said below
- k_gain: float32 [64], replicated, may hold values from 0.4 to 14, as said below
- w_out: bfloat16 [1024, 2048], P('tp'), may hold values from -0.1875 to 0.1875
Outputs:
- mixed: bfloat16 [8, 4096, 2048], P('dp', ('sp', 'tp'))
The draws below stay inside these ranges and needn't reach their ends.
Inputs may be any that keep to these rules, and one draw needn't show every extreme that they name: `q_gain`: gains of the normalized query channels. `k_gain`: gains of the normalized key channels.
All inputs are finite; a program needn't handle non-finite values.
Results may differ from the reference program's by a relative error of at most 0.015.
The reference program's roundings to bfloat16 on the way count: a program that leaves them out, or rounds other values in their place, can miss the bound.
Values may be sent and summed in bfloat16 or wider, within the bound.
No kernel may reach another device: no remote copies, remote signals or barrier semaphores. Data moves between devices by JAX's collectives and lax.ppermute only.
A program may use at most 64 MiB of HBM per device.

```python
import jax
import jax.numpy as jnp
from jax import lax

D = 2048
HEADS = 16
KV_HEADS = 4
HEAD_DIM = 64
GRID_W = 64
TOKENS = 4096
CTX = 512
SAMPLES = 8
GROUPS = 4


def gain_common(key, salt):
    own_key = jax.random.fold_in(key, salt)
    return jax.random.uniform(own_key, (HEAD_DIM,), jnp.float32, 0.4, 1.8)


def draw_q_gain(key, part):
    return gain_common(key, 21)


def draw_k_gain(key, part):
    return gain_common(key, 22)


def level_of(stream_key, shape, pieces, least, largest):
    loudness, own = 1.0, jax.random.fold_in(stream_key, 6)
    for position, parts in pieces:
        heights = jnp.exp(jax.random.uniform(jax.random.fold_in(own, position), (parts,), jnp.float32, least / len(pieces), largest / len(pieces)))
        loudness = loudness * jnp.repeat(heights, shape[position] // parts).reshape([-1 if axis == position else 1 for axis in range(len(shape))])
    return loudness


def centred(stream_key, dims, width, bound, cuts=(), kind=jnp.bfloat16):
    drawn = jax.random.normal(stream_key, dims, jnp.float32) * width
    if len(cuts) > 0:
        drawn = level_of(stream_key, dims, cuts, -0.22, 0.18) * drawn
    return jnp.clip(drawn, min=-bound, max=bound).astype(kind)


def setup_inputs(seed: int = 0) -> dict:
    keys = jax.random.split(jax.random.key(seed), 12)
    return {
        "latent": centred(keys[0], (SAMPLES, TOKENS, D), 1.0, 6.0, ((0, 8), (1, 16))),
        "context": centred(keys[1], (SAMPLES, CTX, D), 1.0, 6.0, ((0, 8), (1, 16))),
        "condition": centred(keys[2], (SAMPLES, D), 1.0, 6.0, ((0, 8),)),
        "mod_weight": centred(keys[3], (D, 3 * D), D ** -0.5, 0.125, ((1, 64),)),
        "norm_gain": jnp.clip(1.0 + 0.18 * jax.random.normal(keys[4], (D,), jnp.float32), 0.1, 1.9),
        "w_query": centred(keys[5], (D, HEADS * HEAD_DIM), D ** -0.5, 0.125, ((1, 4),)),
        "w_key": centred(keys[6], (D, KV_HEADS * HEAD_DIM), D ** -0.5, 0.125, ((1, 4),)),
        "w_value": centred(keys[7], (D, KV_HEADS * HEAD_DIM), D ** -0.5, 0.125, ((1, 4),)),
        "q_gain": draw_q_gain(jax.random.fold_in(keys[11], 71), 0),
        "k_gain": draw_k_gain(jax.random.fold_in(keys[11], 71), 0),
        "w_out": centred(keys[10], (HEADS * HEAD_DIM, D), (HEADS * HEAD_DIM) ** -0.5, 0.1875, ((0, 4),)),
    }


epsilon = 1e-06
rope_base = 10000.0

def normalize(values, gain):
    mean_sq = lax.optimization_barrier(jnp.mean(values * values, axis=-1, keepdims=True))
    return values * lax.rsqrt(mean_sq + epsilon) * gain

def angle_tables(count):
    where = jnp.arange(count, dtype=jnp.int32)
    grid_row = (where // GRID_W).astype(jnp.float32)
    grid_col = (where % GRID_W).astype(jnp.float32)
    quarter = HEAD_DIM // 4
    freqs = rope_base ** (-jnp.arange(quarter, dtype=jnp.float32) / quarter)
    by_row = grid_row[:, None] * freqs[None, :]
    by_col = grid_col[:, None] * freqs[None, :]
    return (jnp.cos(by_row), jnp.sin(by_row), jnp.cos(by_col), jnp.sin(by_col))

def turn_half(values, cosine, sine):
    first, second = jnp.split(values, 2, axis=-1)
    return jnp.concatenate([first * cosine - second * sine, first * sine + second * cosine], axis=-1)

def rotary(values, tables):
    row_cos, row_sin, col_cos, col_sin = tables
    by_row, by_col = jnp.split(values, 2, axis=-1)
    return jnp.concatenate([turn_half(by_row, row_cos, row_sin), turn_half(by_col, col_cos, col_sin)], axis=-1)

def one_sample(latent_one, context_one, modulation_one, norm_gain, w_query, w_key, w_value, q_gain, k_gain, w_out, tables):
    shift = modulation_one[:D]
    scale = modulation_one[D:2 * D]
    gate = modulation_one[2 * D:]
    widened = latent_one.astype(jnp.float32)
    hidden = (normalize(widened, norm_gain) * (1.0 + scale) + shift).astype(jnp.bfloat16)
    queries = jnp.dot(hidden, w_query, preferred_element_type=jnp.float32).reshape(TOKENS, HEADS, HEAD_DIM)
    queries = jnp.transpose(queries, (1, 0, 2))
    queries = rotary(normalize(queries, q_gain), tables).astype(jnp.bfloat16)
    latent_k = jnp.dot(hidden, w_key, preferred_element_type=jnp.float32).reshape(TOKENS, KV_HEADS, HEAD_DIM)
    latent_k = rotary(normalize(jnp.transpose(latent_k, (1, 0, 2)), k_gain), tables).astype(jnp.bfloat16)
    latent_v = jnp.dot(hidden, w_value, preferred_element_type=jnp.float32).astype(jnp.bfloat16)
    latent_v = jnp.transpose(latent_v.reshape(TOKENS, KV_HEADS, HEAD_DIM), (1, 0, 2))
    context_k = jnp.dot(context_one, w_key, preferred_element_type=jnp.float32).reshape(CTX, KV_HEADS, HEAD_DIM)
    context_k = normalize(jnp.transpose(context_k, (1, 0, 2)), k_gain).astype(jnp.bfloat16)
    context_v = jnp.dot(context_one, w_value, preferred_element_type=jnp.float32).astype(jnp.bfloat16)
    context_v = jnp.transpose(context_v.reshape(CTX, KV_HEADS, HEAD_DIM), (1, 0, 2))
    all_keys = jnp.concatenate([context_k, latent_k], axis=1)
    all_values = jnp.concatenate([context_v, latent_v], axis=1)
    group_size = HEADS // KV_HEADS
    score_scale = HEAD_DIM ** (-0.5)

    def one_head(head):
        query_head = lax.dynamic_index_in_dim(queries, head, 0, keepdims=False)
        key_head = lax.dynamic_index_in_dim(all_keys, head // group_size, 0, keepdims=False)
        value_head = lax.dynamic_index_in_dim(all_values, head // group_size, 0, keepdims=False)
        scores = jnp.dot(query_head, key_head.T, preferred_element_type=jnp.float32) * score_scale
        unrounded = jnp.exp(scores - lax.optimization_barrier(jnp.max(scores, axis=-1, keepdims=True)))
        total = lax.optimization_barrier(jnp.sum(unrounded, axis=-1, keepdims=True))
        weights = unrounded.astype(jnp.bfloat16)
        summed = jnp.dot(weights, value_head, preferred_element_type=jnp.float32)
        return (summed / total).astype(jnp.bfloat16)
    attended = lax.map(one_head, jnp.arange(HEADS, dtype=jnp.int32))
    attended = jnp.transpose(attended, (1, 0, 2)).reshape(TOKENS, GROUPS, HEADS * HEAD_DIM // GROUPS)
    out_groups = w_out.reshape(GROUPS, HEADS * HEAD_DIM // GROUPS, D)
    partial_value = jnp.einsum('tgf,gfd->gtd', attended.astype(jnp.float32), out_groups.astype(jnp.float32))
    partial_value = lax.optimization_barrier(partial_value.astype(jnp.bfloat16)).astype(jnp.float32)
    projected = lax.optimization_barrier(jnp.sum(partial_value, axis=0))
    return (widened + gate * projected).astype(jnp.bfloat16)

def reference(latent, context, condition, mod_weight, norm_gain, w_query, w_key, w_value, q_gain, k_gain, w_out):
    cond_act = jax.nn.silu(condition.astype(jnp.float32)).astype(jnp.bfloat16)
    modulation = jnp.dot(cond_act, mod_weight, preferred_element_type=jnp.float32)
    tables = angle_tables(TOKENS)

    def per_sample(index):
        latent_one = lax.dynamic_index_in_dim(latent, index, 0, keepdims=False)
        context_one = lax.dynamic_index_in_dim(context, index, 0, keepdims=False)
        modulation_one = lax.dynamic_index_in_dim(modulation, index, 0, keepdims=False)
        return one_sample(latent_one, context_one, modulation_one, norm_gain, w_query, w_key, w_value, q_gain, k_gain, w_out, tables)
    return lax.map(per_sample, jnp.arange(SAMPLES, dtype=jnp.int32))
```

```python
import functools

import jax
import jax.numpy as jnp
from jax import lax
from jax.experimental import pallas as pl
from jax.experimental.pallas import tpu as pltpu
from jax.sharding import PartitionSpec as P

GRID_W = 64
LANES = 128
KEY_STEP = 512

epsilon = 1e-06
rope_base = 10000.0


def copy_for_each(shard, axis):
    devices = lax.axis_size(axis)
    return lax.all_to_all(
        jnp.broadcast_to(shard[None], (devices, *shard.shape)), axis, 0, 0, tiled=True
    )


def rotary_tables(first, rows, extra, head_dim):
    shape = (rows + extra, LANES)
    row = lax.broadcasted_iota(jnp.int32, shape, 0)
    lane = lax.broadcasted_iota(jnp.int32, shape, 1)
    where = first + row
    quarter = head_dim // 4
    place = jnp.where(lane % head_dim < head_dim // 2, where // GRID_W, where % GRID_W)
    place = jnp.where(row < rows, place, 0)
    freqs = rope_base ** (-(lane % quarter).astype(jnp.float32) / quarter)
    angle = place.astype(jnp.float32) * freqs
    sine = jnp.sin(angle)
    return jnp.cos(angle), jnp.where(lane % (2 * quarter) < quarter, -sine, sine)


def project(
    lat_ref,
    ctx_ref,
    mod_ref,
    gain_ref,
    wq_ref,
    wk_ref,
    wv_ref,
    qg_ref,
    kg_ref,
    cos_ref,
    sin_ref,
    q_ref,
    kv_ref,
    gate_ref,
    hid_ref,
    mods_ref,
):
    rows, width = lat_ref.shape
    count = ctx_ref.shape[0]
    head_dim = qg_ref.shape[1]
    pieces, _, piece = mod_ref.shape
    for j in range(pieces):
        mods_ref[0:1, piece * j : piece * (j + 1)] = mod_ref[j]
    shift = mods_ref[0:1, 0:width]
    scale = 1.0 + mods_ref[0:1, width : 2 * width]
    gate_ref[...] = mods_ref[0:1, 2 * width : 3 * width]
    gain = gain_ref[...]
    step = 32
    for r in range(0, rows, step):
        x = lat_ref[r : r + step, :].astype(jnp.float32)
        mean_sq = jnp.mean(x * x, axis=-1, keepdims=True)
        hidden = x * lax.rsqrt(mean_sq + epsilon) * gain * scale + shift
        hid_ref[r : r + step, :] = hidden.astype(jnp.bfloat16)
    hid_ref[rows:, :] = ctx_ref[...]

    lane = lax.broadcasted_iota(jnp.int32, (1, LANES), 1)
    low = lane < head_dim
    first = lane % (head_dim // 2) < head_dim // 4
    a = lax.broadcasted_iota(jnp.int32, (LANES, LANES), 0) // head_dim
    b = lax.broadcasted_iota(jnp.int32, (LANES, LANES), 1) // head_dim
    average = jnp.where(a == b, 1.0 / head_dim, 0.0).astype(jnp.float32)

    def turned(values, gains, cosine, sine):
        mean_sq = jnp.dot(
            values * values,
            average,
            preferred_element_type=jnp.float32,
            precision=lax.Precision.HIGHEST,
        )
        values = values * lax.rsqrt(mean_sq + epsilon) * gains
        ahead = pltpu.roll(values, LANES - head_dim // 4, 1)
        behind = pltpu.roll(values, head_dim // 4, 1)
        return values * cosine + jnp.where(first, ahead, behind) * sine

    qg = jnp.concatenate([qg_ref[...]] * 2, axis=1)
    kg = jnp.concatenate([kg_ref[...]] * 2, axis=1)
    cosine, sine = cos_ref[...], sin_ref[...]
    hid = hid_ref[...]
    keys = jnp.dot(hid, wk_ref[...], preferred_element_type=jnp.float32)
    values = jnp.dot(hid, wv_ref[...], preferred_element_type=jnp.float32)
    both = jnp.concatenate([keys, values], axis=1)
    kv_ref[...] = jnp.where(low, turned(both, kg, cosine, sine), both).astype(jnp.bfloat16)
    queries = jnp.dot(hid[:rows], wq_ref[...], preferred_element_type=jnp.float32)
    zero = jnp.zeros((), jnp.bfloat16)
    for g in range(queries.shape[1] // LANES):
        pair = turned(
            queries[:, LANES * g : LANES * (g + 1)], qg, cosine[:rows], sine[:rows]
        )
        pair = pair.astype(jnp.bfloat16).astype(jnp.float32) * head_dim**-0.5
        other = pltpu.roll(pair, head_dim, 1)
        q_ref[2 * g] = jnp.where(low, pair, 0.0).astype(jnp.bfloat16)
        q_ref[2 * g + 1] = jnp.where(low, other, 0.0).astype(jnp.bfloat16)


def attend(q_ref, kv_ref, o_ref, s_ref):
    heads, rows, _ = q_ref.shape
    head_dim = o_ref.shape[1] // heads
    total_keys = kv_ref.shape[0]
    steps = total_keys // KEY_STEP
    for h in range(heads):
        q = q_ref[h]
        m = jnp.full((rows, LANES), -jnp.inf, jnp.float32)
        for c in range(steps):
            part = slice(c * KEY_STEP, (c + 1) * KEY_STEP)
            s = lax.dot_general(
                q, kv_ref[part, :], (((1,), (1,)), ((), ())), preferred_element_type=jnp.float32
            )
            s_ref[h % 2, :, part] = s
            for j in range(0, KEY_STEP, LANES):
                m = jnp.maximum(m, s[:, j : j + LANES])
        row_max = jnp.max(m, axis=1, keepdims=True)
        total = jnp.zeros((rows, LANES), jnp.float32)
        acc = jnp.zeros((rows, LANES), jnp.float32)
        for c in range(steps):
            part = slice(c * KEY_STEP, (c + 1) * KEY_STEP)
            p = jnp.exp(s_ref[h % 2, :, part] - row_max)
            for j in range(0, KEY_STEP, LANES):
                total = total + p[:, j : j + LANES]
            acc = acc + jnp.dot(
                p.astype(jnp.bfloat16), kv_ref[part, :], preferred_element_type=jnp.float32
            )
        total = jnp.sum(total, axis=1, keepdims=True)
        o_ref[:, head_dim * h : head_dim * (h + 1)] = (acc[:, head_dim:] / total).astype(
            jnp.bfloat16
        )


def finish(at_ref, att_ref, w_ref, lat_ref, gate_ref, out_ref):
    projected = 0.0
    for g in range(att_ref.shape[0]):
        term = jnp.dot(att_ref[g], w_ref[g], preferred_element_type=jnp.float32)
        projected = projected + term.astype(jnp.bfloat16).astype(jnp.float32)
    residual = lat_ref[...].astype(jnp.float32)
    out_ref[...] = (residual + gate_ref[...] * projected).astype(jnp.bfloat16)


def shards(
    latent,
    context,
    condition,
    mod_weight,
    norm_gain,
    w_query,
    w_key,
    w_value,
    q_gain,
    k_gain,
    w_out,
):
    _, length, width = latent.shape
    count = context.shape[1]
    head_dim = q_gain.shape[0]
    heads = w_query.shape[1] // head_dim
    sp, tp = lax.axis_size("sp"), lax.axis_size("tp")
    cond_act = jax.nn.silu(condition.astype(jnp.float32)).astype(jnp.bfloat16)
    mod_piece = jnp.dot(cond_act, mod_weight, preferred_element_type=jnp.float32)
    modulation = copy_for_each(mod_piece, ("sp", "tp"))
    cosine, sine = rotary_tables(lax.axis_index("sp") * length, length, count, head_dim)

    queries, own_kv, gate = pl.pallas_call(
        project,
        out_shape=(
            jax.ShapeDtypeStruct((heads, length, LANES), jnp.bfloat16),
            jax.ShapeDtypeStruct((length + count, LANES), jnp.bfloat16),
            jax.ShapeDtypeStruct((1, width), jnp.float32),
        ),
        scratch_shapes=[
            pltpu.VMEM((length + count, width), jnp.bfloat16),
            pltpu.VMEM((8, 3 * width), jnp.float32),
        ],
        compiler_params=pltpu.CompilerParams(vmem_limit_bytes=40 * 2**20),
        name="project",
    )(
        latent[0],
        context[0],
        modulation,
        norm_gain[None],
        w_query,
        w_key,
        w_value,
        q_gain[None],
        k_gain[None],
        cosine,
        sine,
    )
    all_kv = copy_for_each(own_kv, "sp").reshape(sp * (length + count), LANES)
    late_w_out, _ = lax.optimization_barrier((w_out, own_kv))
    whole_w_out = copy_for_each(late_w_out, "tp")
    attended = pl.pallas_call(
        attend,
        out_shape=jax.ShapeDtypeStruct((length, heads * head_dim), jnp.bfloat16),
        scratch_shapes=[pltpu.VMEM((2, length, all_kv.shape[0]), jnp.float32)],
        compiler_params=pltpu.CompilerParams(vmem_limit_bytes=40 * 2**20),
        name="attend",
    )(queries, all_kv)
    kept = length // tp
    attended = lax.all_to_all(
        attended.reshape(tp, kept, heads * head_dim), "tp", 0, 0, tiled=True
    )
    cols = 512
    mixed = pl.pallas_call(
        finish,
        grid_spec=pltpu.PrefetchScalarGridSpec(
            num_scalar_prefetch=1,
            grid=(width // cols,),
            in_specs=[
                pl.BlockSpec((tp, kept, heads * head_dim), lambda i, at: (0, 0, 0)),
                pl.BlockSpec((tp, heads * head_dim, cols), lambda i, at: (0, 0, i)),
                pl.BlockSpec((kept, cols), lambda i, at: (at[0], i)),
                pl.BlockSpec((1, cols), lambda i, at: (0, i)),
            ],
            out_specs=pl.BlockSpec((kept, cols), lambda i, at: (0, i)),
        ),
        out_shape=jax.ShapeDtypeStruct((kept, width), jnp.bfloat16),
        name="finish",
    )(lax.axis_index("tp").astype(jnp.int32)[None], attended, whole_w_out, latent[0], gate)
    return mixed[None]


def solution(mesh):
    placed = (
        P("dp", "sp", None),
        P("dp", "sp", None),
        P("dp", None),
        P(None, ("sp", "tp")),
        P(),
        P(None, "tp"),
        P(None, "tp"),
        P(None, "tp"),
        P(),
        P(),
        P("tp", None),
    )
    return jax.shard_map(
        shards, mesh=mesh, in_specs=placed, out_specs=P("dp", ("sp", "tp"), None), check_vma=False
    )
```

```python
import jax
import jax.numpy as jnp
from jax import lax
from jax.experimental import pallas as pl
from jax.experimental.pallas import tpu as pltpu
from jax.sharding import PartitionSpec as P

GRID_W = 64
LANES = 128
KEY_STEP = 512

epsilon = 1e-06
rope_base = 10000.0


def copy_for_each(shard, axis):
    devices = lax.axis_size(axis)
    return lax.all_to_all(
        jnp.broadcast_to(shard[None], (devices, *shard.shape)), axis, 0, 0, tiled=True
    )


def rotary_tables(first, rows, extra, head_dim):
    shape = (rows + extra, LANES)
    row = lax.broadcasted_iota(jnp.int32, shape, 0)
    lane = lax.broadcasted_iota(jnp.int32, shape, 1)
    where = first + row
    quarter = head_dim // 4
    place = jnp.where(lane % head_dim < head_dim // 2, where // GRID_W, where % GRID_W)
    place = jnp.where(row < rows, place, 0)
    freqs = rope_base ** (-(lane % quarter).astype(jnp.float32) / quarter)
    angle = place.astype(jnp.float32) * freqs
    sine = jnp.sin(angle)
    return jnp.cos(angle), jnp.where(lane % (2 * quarter) < quarter, -sine, sine)


def turner(head_dim):
    lane = lax.broadcasted_iota(jnp.int32, (1, LANES), 1)
    first = lane % (head_dim // 2) < head_dim // 4
    a = lax.broadcasted_iota(jnp.int32, (LANES, LANES), 0) // head_dim
    b = lax.broadcasted_iota(jnp.int32, (LANES, LANES), 1) // head_dim
    average = jnp.where(a == b, 1.0 / head_dim, 0.0).astype(jnp.float32)

    def scaled(values, gains):
        mean_sq = jnp.dot(
            values * values,
            average,
            preferred_element_type=jnp.float32,
            precision=lax.Precision.HIGHEST,
        )
        return values * lax.rsqrt(mean_sq + epsilon) * gains

    def turned(values, cosine, sine):
        ahead = pltpu.roll(values, LANES - head_dim // 4, 1)
        behind = pltpu.roll(values, head_dim // 4, 1)
        return values * cosine + jnp.where(first, ahead, behind) * sine

    return scaled, turned, lane < head_dim


def contract_last(a, b):
    return lax.dot_general(a, b, (((1,), (1,)), ((), ())), preferred_element_type=jnp.float32)


def start_all(pairs, sems):
    copies = [pltpu.make_async_copy(a, b, sems.at[i]) for i, (a, b) in enumerate(pairs)]
    for copy in copies:
        copy.start()
    return copies


def prepare(
    lat_hbm, ctx_hbm, wk_hbm, wv_hbm, kg_ref, inv_ref, ctx_kv_ref, lat_ref, ctx_ref, wkv_ref, sems
):
    rows = lat_ref.shape[0]
    head_dim = kg_ref.shape[1]
    copies = start_all(
        (
            (lat_hbm, lat_ref),
            (ctx_hbm, ctx_ref),
            (wk_hbm, wkv_ref.at[pl.ds(0, head_dim)]),
            (wv_hbm, wkv_ref.at[pl.ds(head_dim, head_dim)]),
        ),
        sems,
    )
    copies[0].wait()
    step = 32
    for r in range(0, rows, step):
        x = lat_ref[r : r + step, :].astype(jnp.float32)
        mean_sq = jnp.mean(x * x, axis=-1, keepdims=True)
        inv_ref[r : r + step, :] = jnp.broadcast_to(lax.rsqrt(mean_sq + epsilon), (step, LANES))
    for copy in copies[1:]:
        copy.wait()
    scaled, _, low = turner(head_dim)
    both = contract_last(ctx_ref[...], wkv_ref[...])
    kg = jnp.concatenate([kg_ref[...]] * 2, axis=1)
    ctx_kv_ref[...] = jnp.where(low, scaled(both, kg), both).astype(jnp.bfloat16)


def project(
    lat_hbm,
    wq_hbm,
    wk_hbm,
    wv_hbm,
    inv_ref,
    ctx_kv_ref,
    mod_ref,
    gain_ref,
    qg_ref,
    kg_ref,
    cos_ref,
    sin_ref,
    q_ref,
    main_ref,
    rest_ref,
    gate_ref,
    lat_ref,
    wq_ref,
    wkv_ref,
    hid_ref,
    mods_ref,
    sems,
):
    rows, width = lat_ref.shape
    main = main_ref.shape[0]
    head_dim = qg_ref.shape[1]
    copies = start_all(
        (
            (lat_hbm, lat_ref),
            (wk_hbm, wkv_ref.at[pl.ds(0, head_dim)]),
            (wv_hbm, wkv_ref.at[pl.ds(head_dim, head_dim)]),
            (wq_hbm, wq_ref),
        ),
        sems,
    )
    pieces, _, piece = mod_ref.shape
    for j in range(pieces):
        mods_ref[0:1, piece * j : piece * (j + 1)] = mod_ref[j]
    shift = mods_ref[0:1, 0:width]
    scale = 1.0 + mods_ref[0:1, width : 2 * width]
    gate_ref[...] = mods_ref[0:1, 2 * width : 3 * width]
    gain = gain_ref[...]
    step = 32
    copies[0].wait()
    for r in range(0, rows, step):
        x = lat_ref[r : r + step, :].astype(jnp.float32)
        hidden = x * inv_ref[r : r + step, 0:1] * gain * scale + shift
        hid_ref[r : r + step, :] = hidden.astype(jnp.bfloat16)

    scaled, turned, low = turner(head_dim)
    qg = jnp.concatenate([qg_ref[...]] * 2, axis=1)
    kg = jnp.concatenate([kg_ref[...]] * 2, axis=1)
    cosine, sine = cos_ref[...], sin_ref[...]
    hid = hid_ref[...]
    copies[1].wait()
    copies[2].wait()
    both = contract_last(hid, wkv_ref[...])
    both = jnp.where(low, turned(scaled(both, kg), cosine, sine), both).astype(jnp.bfloat16)
    main_ref[...] = both[:main]
    rest_ref[0 : rows - main, :] = both[main:]
    rest_ref[rows - main :, :] = ctx_kv_ref[...]
    copies[3].wait()
    queries = jnp.dot(hid, wq_ref[...], preferred_element_type=jnp.float32)
    for g in range(queries.shape[1] // LANES):
        pair = turned(scaled(queries[:, LANES * g : LANES * (g + 1)], qg), cosine, sine)
        pair = pair.astype(jnp.bfloat16).astype(jnp.float32) * head_dim**-0.5
        other = pltpu.roll(pair, head_dim, 1)
        q_ref[2 * g] = jnp.where(low, pair, 0.0).astype(jnp.bfloat16)
        q_ref[2 * g + 1] = jnp.where(low, other, 0.0).astype(jnp.bfloat16)


def attend(q_hbm, main_ref, rest_ref, w_hbm, o_ref, q_ref, s_ref, at_ref, w_ref, sems):
    copies = start_all(((q_hbm, q_ref), (w_hbm, w_ref)), sems)
    heads, rows, _ = q_ref.shape
    head_dim = at_ref.shape[1] // heads
    parts, at = [], 0
    for ref in (main_ref, rest_ref):
        count = ref.shape[0]
        for c in range(0, count, KEY_STEP):
            size = min(KEY_STEP, count - c)
            parts.append((ref, c, at, size))
            at += size
    copies[0].wait()
    for h in range(heads):
        q = q_ref[h]
        m = jnp.full((rows, LANES), -jnp.inf, jnp.float32)
        for ref, c, at, size in parts:
            s = contract_last(q, ref[c : c + size, :])
            s_ref[h % 2, :, at : at + size] = s
            for j in range(0, size, LANES):
                m = jnp.maximum(m, s[:, j : j + LANES])
        row_max = jnp.max(m, axis=1, keepdims=True)
        total = jnp.zeros((rows, LANES), jnp.float32)
        acc = jnp.zeros((rows, LANES), jnp.float32)
        for ref, c, at, size in parts:
            p = jnp.exp(s_ref[h % 2, :, at : at + size] - row_max)
            for j in range(0, size, LANES):
                total = total + p[:, j : j + LANES]
            acc = acc + jnp.dot(
                p.astype(jnp.bfloat16), ref[c : c + size, :], preferred_element_type=jnp.float32
            )
        total = jnp.sum(total, axis=1, keepdims=True)
        at_ref[:, head_dim * h : head_dim * (h + 1)] = (acc[:, head_dim:] / total).astype(
            jnp.bfloat16
        )
    copies[1].wait()
    o_ref[...] = jnp.dot(at_ref[...], w_ref[...], preferred_element_type=jnp.float32).astype(
        jnp.bfloat16
    )


def finish(at_ref, lat_hbm, terms_ref, gate_ref, out_ref, kept_ref, sems):
    kept = kept_ref.shape[0]
    at = pl.multiple_of(at_ref[0] * kept, kept)
    (copy,) = start_all(((lat_hbm.at[pl.ds(at, kept)], kept_ref),), sems)
    projected = terms_ref[0].astype(jnp.float32)
    for g in range(1, terms_ref.shape[0]):
        projected = projected + terms_ref[g].astype(jnp.float32)
    copy.wait()
    residual = kept_ref[...].astype(jnp.float32)
    out_ref[...] = (residual + gate_ref[...] * projected).astype(jnp.bfloat16)


def vmem(mebibytes):
    return pltpu.CompilerParams(vmem_limit_bytes=mebibytes * 2**20)


def in_vmem(count):
    return [pl.BlockSpec(memory_space=pltpu.VMEM)] * count


def in_hbm(count):
    return [pl.BlockSpec(memory_space=pltpu.HBM)] * count


def shards(
    latent,
    context,
    condition,
    mod_weight,
    norm_gain,
    w_query,
    w_key,
    w_value,
    q_gain,
    k_gain,
    w_out,
):
    _, length, width = latent.shape
    count = context.shape[1]
    head_dim = q_gain.shape[0]
    heads = w_query.shape[1] // head_dim
    sp, tp = lax.axis_size("sp"), lax.axis_size("tp")
    kept = length // tp
    main = length - 8
    rest = length - main + count
    half, single = jnp.bfloat16, jnp.float32
    shape = jax.ShapeDtypeStruct
    cond_act = jax.nn.silu(condition.astype(jnp.float32)).astype(jnp.bfloat16)
    mod_piece = jnp.dot(cond_act, mod_weight, preferred_element_type=jnp.float32)
    modulation = copy_for_each(mod_piece, ("sp", "tp"))
    cosine, sine = rotary_tables(lax.axis_index("sp") * length, length, 0, head_dim)

    dma = lambda count: pltpu.SemaphoreType.DMA((count,))
    wk, wv = w_key.T, w_value.T
    inverse, ctx_kv = pl.pallas_call(
        prepare,
        out_shape=(shape((length, LANES), single), shape((count, LANES), half)),
        in_specs=in_hbm(4) + in_vmem(1),
        scratch_shapes=[
            pltpu.VMEM((length, width), half),
            pltpu.VMEM((count, width), half),
            pltpu.VMEM((2 * head_dim, width), half),
            dma(4),
        ],
        compiler_params=vmem(12),
        name="prepare",
    )(latent[0], context[0], wk, wv, k_gain[None])
    queries, own_main, own_rest, gate = pl.pallas_call(
        project,
        out_shape=(
            shape((heads, length, LANES), half),
            shape((main, LANES), half),
            shape((rest, LANES), half),
            shape((1, width), single),
        ),
        in_specs=in_hbm(4) + in_vmem(8),
        scratch_shapes=[
            pltpu.VMEM((length, width), half),
            pltpu.VMEM(w_query.shape, half),
            pltpu.VMEM((2 * head_dim, width), half),
            pltpu.VMEM((length, width), half),
            pltpu.VMEM((8, 3 * width), single),
            dma(4),
        ],
        compiler_params=vmem(16),
        name="project",
    )(
        latent[0],
        w_query,
        wk,
        wv,
        inverse,
        ctx_kv,
        modulation,
        norm_gain[None],
        q_gain[None],
        k_gain[None],
        cosine,
        sine,
    )
    all_rest = copy_for_each(own_rest, "sp").reshape(sp * rest, LANES)
    all_main = lax.all_gather(own_main, "sp", axis=0, tiled=True)
    all_keys = sp * (main + rest)
    terms = pl.pallas_call(
        attend,
        out_shape=shape((length, width), half),
        in_specs=in_hbm(1) + in_vmem(2) + in_hbm(1),
        scratch_shapes=[
            pltpu.VMEM((heads, length, LANES), half),
            pltpu.VMEM((2, length, all_keys), single),
            pltpu.VMEM((length, heads * head_dim), half),
            pltpu.VMEM(w_out.shape, half),
            dma(2),
        ],
        compiler_params=vmem(32),
        name="attend",
    )(queries, all_main, all_rest, w_out)
    terms = lax.all_to_all(terms.reshape(tp, kept, width), "tp", 0, 0, tiled=True)
    mixed = pl.pallas_call(
        finish,
        out_shape=shape((kept, width), half),
        in_specs=[pl.BlockSpec(memory_space=pltpu.SMEM)] + in_hbm(1) + in_vmem(2),
        scratch_shapes=[pltpu.VMEM((kept, width), half), dma(1)],
        compiler_params=vmem(8),
        name="finish",
    )(lax.axis_index("tp").astype(jnp.int32)[None], latent[0], terms, gate)
    return mixed[None]


def solution(mesh):
    placed = (
        P("dp", "sp", None),
        P("dp", "sp", None),
        P("dp", None),
        P(None, ("sp", "tp")),
        P(),
        P(None, "tp"),
        P(None, "tp"),
        P(None, "tp"),
        P(),
        P(),
        P("tp", None),
    )
    return jax.shard_map(
        shards, mesh=mesh, in_specs=placed, out_specs=P("dp", ("sp", "tp"), None), check_vma=False
    )
```

```python
import jax
import jax.numpy as jnp
from jax import lax
from jax.experimental import pallas as pl
from jax.experimental.pallas import tpu as pltpu
from jax.sharding import PartitionSpec as P

GRID_W = 64
LANES = 128
KEY_STEP = 512

epsilon = 1e-06
rope_base = 10000.0


def rotary_tables(first, rows, extra, head_dim):
    shape = (rows + extra, LANES)
    row = lax.broadcasted_iota(jnp.int32, shape, 0)
    lane = lax.broadcasted_iota(jnp.int32, shape, 1)
    where = first + row
    quarter = head_dim // 4
    place = jnp.where(lane % head_dim < head_dim // 2, where // GRID_W, where % GRID_W)
    place = jnp.where(row < rows, place, 0)
    freqs = rope_base ** (-(lane % quarter).astype(jnp.float32) / quarter)
    angle = place.astype(jnp.float32) * freqs
    sine = jnp.sin(angle)
    return jnp.cos(angle), jnp.where(lane % (2 * quarter) < quarter, -sine, sine)


def turner(head_dim):
    lane = lax.broadcasted_iota(jnp.int32, (1, LANES), 1)
    first = lane % (head_dim // 2) < head_dim // 4
    a = lax.broadcasted_iota(jnp.int32, (LANES, LANES), 0) // head_dim
    b = lax.broadcasted_iota(jnp.int32, (LANES, LANES), 1) // head_dim
    average = jnp.where(a == b, 1.0 / head_dim, 0.0).astype(jnp.float32)

    def scaled(values, gains):
        mean_sq = jnp.dot(
            values * values,
            average,
            preferred_element_type=jnp.float32,
            precision=lax.Precision.HIGHEST,
        )
        return values * lax.rsqrt(mean_sq + epsilon) * gains

    def turned(values, cosine, sine):
        ahead = pltpu.roll(values, LANES - head_dim // 4, 1)
        behind = pltpu.roll(values, head_dim // 4, 1)
        return values * cosine + jnp.where(first, ahead, behind) * sine

    return scaled, turned, lane < head_dim


def contract_last(a, b):
    return lax.dot_general(a, b, (((1,), (1,)), ((), ())), preferred_element_type=jnp.float32)


def start_all(pairs, sems):
    copies = [pltpu.make_async_copy(a, b, sems.at[i]) for i, (a, b) in enumerate(pairs)]
    for copy in copies:
        copy.start()
    return copies


def modulate(cond_ref, w_hbm, out_ref, w_ref, sems):
    (copy,) = start_all(((w_hbm, w_ref),), sems)
    cond = cond_ref[...].astype(jnp.float32)
    active = (cond / (1.0 + jnp.exp(-cond))).astype(jnp.bfloat16)
    active = jnp.broadcast_to(active, (16, active.shape[1]))
    copy.wait()
    piece = contract_last(active, w_ref[...])[0:1]
    out_ref[...] = jnp.broadcast_to(piece[None], out_ref.shape)


def prepare(
    lat_hbm, ctx_hbm, wk_hbm, wv_hbm, kg_ref, inv_ref, ctx_kv_ref, lat_ref, ctx_ref, wkv_ref, sems
):
    rows = lat_ref.shape[0]
    head_dim = kg_ref.shape[1]
    copies = start_all(
        (
            (lat_hbm, lat_ref),
            (ctx_hbm, ctx_ref),
            (wk_hbm, wkv_ref.at[pl.ds(0, head_dim)]),
            (wv_hbm, wkv_ref.at[pl.ds(head_dim, head_dim)]),
        ),
        sems,
    )
    copies[0].wait()
    step = 32
    for r in range(0, rows, step):
        x = lat_ref[r : r + step, :].astype(jnp.float32)
        mean_sq = jnp.mean(x * x, axis=-1, keepdims=True)
        inv_ref[r : r + step, :] = jnp.broadcast_to(lax.rsqrt(mean_sq + epsilon), (step, LANES))
    for copy in copies[1:]:
        copy.wait()
    scaled, _, low = turner(head_dim)
    both = contract_last(ctx_ref[...], wkv_ref[...])
    kg = jnp.concatenate([kg_ref[...]] * 2, axis=1)
    ctx_kv_ref[...] = jnp.where(low, scaled(both, kg), both).astype(jnp.bfloat16)


def project(
    lat_hbm,
    wq_hbm,
    wk_hbm,
    wv_hbm,
    inv_ref,
    ctx_kv_ref,
    mod_ref,
    gain_ref,
    qg_ref,
    kg_ref,
    cos_ref,
    sin_ref,
    q_hbm,
    main_hbm,
    rest_hbm,
    gate_ref,
    lat_ref,
    wq_ref,
    wkv_ref,
    hid_ref,
    mods_ref,
    q_ref,
    kv_ref,
    sems,
    out_sems,
):
    rows, width = lat_ref.shape
    main = main_hbm.shape[0]
    rest = rest_hbm.shape[1]
    head_dim = qg_ref.shape[1]
    copies = start_all(
        (
            (lat_hbm, lat_ref),
            (wk_hbm, wkv_ref.at[pl.ds(0, head_dim)]),
            (wv_hbm, wkv_ref.at[pl.ds(head_dim, head_dim)]),
            (wq_hbm, wq_ref),
        ),
        sems,
    )
    pieces, _, piece = mod_ref.shape
    for j in range(pieces):
        mods_ref[0:1, piece * j : piece * (j + 1)] = mod_ref[j]
    shift = mods_ref[0:1, 0:width]
    scale = 1.0 + mods_ref[0:1, width : 2 * width]
    gate_ref[...] = mods_ref[0:1, 2 * width : 3 * width]
    gain = gain_ref[...]
    step = 32
    copies[0].wait()
    for r in range(0, rows, step):
        x = lat_ref[r : r + step, :].astype(jnp.float32)
        hidden = x * inv_ref[r : r + step, 0:1] * gain * scale + shift
        hid_ref[r : r + step, :] = hidden.astype(jnp.bfloat16)

    scaled, turned, low = turner(head_dim)
    qg = jnp.concatenate([qg_ref[...]] * 2, axis=1)
    kg = jnp.concatenate([kg_ref[...]] * 2, axis=1)
    cosine, sine = cos_ref[...], sin_ref[...]
    hid = hid_ref[...]
    copies[1].wait()
    copies[2].wait()
    both = contract_last(hid, wkv_ref[...])
    both = jnp.where(low, turned(scaled(both, kg), cosine, sine), both).astype(jnp.bfloat16)
    kv_ref[0:rows, :] = both
    kv_ref[rows:, :] = ctx_kv_ref[...]
    sent = kv_ref.at[pl.ds(main, rest)]
    outs = start_all(
        [(kv_ref.at[pl.ds(0, main)], main_hbm)]
        + [(sent, rest_hbm.at[z]) for z in range(rest_hbm.shape[0])],
        out_sems,
    )
    copies[3].wait()
    queries = jnp.dot(hid, wq_ref[...], preferred_element_type=jnp.float32)
    for g in range(queries.shape[1] // LANES):
        pair = turned(scaled(queries[:, LANES * g : LANES * (g + 1)], qg), cosine, sine)
        pair = pair.astype(jnp.bfloat16).astype(jnp.float32) * head_dim**-0.5
        other = pltpu.roll(pair, head_dim, 1)
        q_ref[2 * g] = jnp.where(low, pair, 0.0).astype(jnp.bfloat16)
        q_ref[2 * g + 1] = jnp.where(low, other, 0.0).astype(jnp.bfloat16)
    last = pltpu.make_async_copy(q_ref, q_hbm, sems.at[4])
    last.start()
    for copy in outs:
        copy.wait()
    last.wait()


def attend(q_hbm, main_ref, rest_ref, w_hbm, o_ref, q_ref, s_ref, at_ref, w_ref, sems):
    copies = start_all(((q_hbm, q_ref), (w_hbm, w_ref)), sems)
    heads, rows, _ = q_ref.shape
    head_dim = at_ref.shape[1] // heads
    parts, at = [], 0
    for ref in (main_ref, rest_ref):
        count = ref.shape[0]
        for c in range(0, count, KEY_STEP):
            size = min(KEY_STEP, count - c)
            parts.append((ref, c, at, size))
            at += size
    copies[0].wait()
    row_max = None
    for h in range(heads + 1):
        if h < heads:
            q = q_ref[h]
            m = jnp.full((rows, LANES), -jnp.inf, jnp.float32)
        if h > 0:
            total = jnp.zeros((rows, LANES), jnp.float32)
            acc = jnp.zeros((rows, LANES), jnp.float32)
        for ref, c, at, size in parts:
            if h < heads:
                s = contract_last(q, ref[c : c + size, :])
                s_ref[h % 2, :, at : at + size] = s
                for j in range(0, size, LANES):
                    m = jnp.maximum(m, s[:, j : j + LANES])
            if h > 0:
                p = jnp.exp(s_ref[(h + 1) % 2, :, at : at + size] - row_max)
                for j in range(0, size, LANES):
                    total = total + p[:, j : j + LANES]
                acc = acc + jnp.dot(
                    p.astype(jnp.bfloat16), ref[c : c + size, :], preferred_element_type=jnp.float32
                )
        if h > 0:
            total = jnp.sum(total, axis=1, keepdims=True)
            at_ref[:, head_dim * (h - 1) : head_dim * h] = (acc[:, head_dim:] / total).astype(
                jnp.bfloat16
            )
        row_max = jnp.max(m, axis=1, keepdims=True)
    copies[1].wait()
    o_ref[...] = jnp.dot(at_ref[...], w_ref[...], preferred_element_type=jnp.float32).astype(
        jnp.bfloat16
    )


def finish(at_ref, lat_hbm, terms_ref, gate_ref, out_ref, kept_ref, sems):
    kept = kept_ref.shape[0]
    at = pl.multiple_of(at_ref[0] * kept, kept)
    (copy,) = start_all(((lat_hbm.at[pl.ds(at, kept)], kept_ref),), sems)
    projected = terms_ref[0].astype(jnp.float32)
    for g in range(1, terms_ref.shape[0]):
        projected = projected + terms_ref[g].astype(jnp.float32)
    copy.wait()
    residual = kept_ref[...].astype(jnp.float32)
    out_ref[...] = (residual + gate_ref[...] * projected).astype(jnp.bfloat16)


def vmem(mebibytes):
    return pltpu.CompilerParams(vmem_limit_bytes=mebibytes * 2**20)


def in_vmem(count):
    return [pl.BlockSpec(memory_space=pltpu.VMEM)] * count


def in_hbm(count):
    return [pl.BlockSpec(memory_space=pltpu.HBM)] * count


def shards(
    latent,
    context,
    condition,
    mod_weight,
    norm_gain,
    w_query,
    w_key,
    w_value,
    q_gain,
    k_gain,
    w_out,
):
    _, length, width = latent.shape
    count = context.shape[1]
    head_dim = q_gain.shape[0]
    heads = w_query.shape[1] // head_dim
    sp, tp = lax.axis_size("sp"), lax.axis_size("tp")
    kept = length // tp
    main = length - 8
    rest = length - main + count
    half, single = jnp.bfloat16, jnp.float32
    shape = jax.ShapeDtypeStruct
    dma = lambda count: pltpu.SemaphoreType.DMA((count,))
    mod_pieces = pl.pallas_call(
        modulate,
        out_shape=shape((sp * tp, 1, mod_weight.shape[1]), single),
        in_specs=in_vmem(1) + in_hbm(1),
        scratch_shapes=[pltpu.VMEM(mod_weight.shape[::-1], half), dma(1)],
        compiler_params=vmem(8),
        name="modulate",
    )(condition, mod_weight.T)
    modulation = lax.all_to_all(mod_pieces, ("sp", "tp"), 0, 0, tiled=True)
    cosine, sine = rotary_tables(lax.axis_index("sp") * length, length, 0, head_dim)

    wk, wv = w_key.T, w_value.T
    inverse, ctx_kv = pl.pallas_call(
        prepare,
        out_shape=(shape((length, LANES), single), shape((count, LANES), half)),
        in_specs=in_hbm(4) + in_vmem(1),
        scratch_shapes=[
            pltpu.VMEM((length, width), half),
            pltpu.VMEM((count, width), half),
            pltpu.VMEM((2 * head_dim, width), half),
            dma(4),
        ],
        compiler_params=vmem(12),
        name="prepare",
    )(latent[0], context[0], wk, wv, k_gain[None])
    queries, own_main, own_rest, gate = pl.pallas_call(
        project,
        out_shape=(
            shape((heads, length, LANES), half),
            shape((main, LANES), half),
            shape((sp, rest, LANES), half),
            shape((1, width), single),
        ),
        in_specs=in_hbm(4) + in_vmem(8),
        out_specs=tuple(in_hbm(3) + in_vmem(1)),
        scratch_shapes=[
            pltpu.VMEM((length, width), half),
            pltpu.VMEM(w_query.shape, half),
            pltpu.VMEM((2 * head_dim, width), half),
            pltpu.VMEM((length, width), half),
            pltpu.VMEM((8, 3 * width), single),
            pltpu.VMEM((heads, length, LANES), half),
            pltpu.VMEM((main + rest, LANES), half),
            dma(5),
            dma(1 + sp),
        ],
        compiler_params=vmem(60),
        name="project",
    )(
        latent[0],
        w_query,
        wk,
        wv,
        inverse,
        ctx_kv,
        modulation,
        norm_gain[None],
        q_gain[None],
        k_gain[None],
        cosine,
        sine,
    )
    all_rest = lax.all_to_all(own_rest, "sp", 0, 0, tiled=True).reshape(sp * rest, LANES)
    all_main = lax.all_gather(own_main, "sp", axis=0, tiled=True)
    all_keys = sp * (main + rest)
    terms = pl.pallas_call(
        attend,
        out_shape=shape((length, width), half),
        in_specs=in_hbm(1) + in_vmem(2) + in_hbm(1),
        scratch_shapes=[
            pltpu.VMEM((heads, length, LANES), half),
            pltpu.VMEM((2, length, all_keys), single),
            pltpu.VMEM((length, heads * head_dim), half),
            pltpu.VMEM(w_out.shape, half),
            dma(2),
        ],
        compiler_params=vmem(32),
        name="attend",
    )(queries, all_main, all_rest, w_out)
    terms = lax.all_to_all(terms.reshape(tp, kept, width), "tp", 0, 0, tiled=True)
    mixed = pl.pallas_call(
        finish,
        out_shape=shape((kept, width), half),
        in_specs=[pl.BlockSpec(memory_space=pltpu.SMEM)] + in_hbm(1) + in_vmem(2),
        scratch_shapes=[pltpu.VMEM((kept, width), half), dma(1)],
        compiler_params=vmem(8),
        name="finish",
    )(lax.axis_index("tp").astype(jnp.int32)[None], latent[0], terms, gate)
    return mixed[None]


def solution(mesh):
    placed = (
        P("dp", "sp", None),
        P("dp", "sp", None),
        P("dp", None),
        P(None, ("sp", "tp")),
        P(),
        P(None, "tp"),
        P(None, "tp"),
        P(None, "tp"),
        P(),
        P(),
        P("tp", None),
    )
    return jax.shard_map(
        shards, mesh=mesh, in_specs=placed, out_specs=P("dp", ("sp", "tp"), None), check_vma=False
    )
```

```python
import jax
import jax.numpy as jnp
from jax import lax
from jax.experimental import pallas as pl
from jax.experimental.pallas import tpu as pltpu
from jax.sharding import PartitionSpec as P


GRID_W = 64
LANES = 128
KEY_STEP = 512

epsilon = 1e-06
rope_base = 10000.0


def rotary_tables(first, rows, extra, head_dim):
    shape = (rows + extra, LANES)
    row = lax.broadcasted_iota(jnp.int32, shape, 0)
    lane = lax.broadcasted_iota(jnp.int32, shape, 1)
    where = first + row
    quarter = head_dim // 4
    place = jnp.where(lane % head_dim < head_dim // 2, where // GRID_W, where % GRID_W)
    place = jnp.where(row < rows, place, 0)
    freqs = rope_base ** (-(lane % quarter).astype(jnp.float32) / quarter)
    angle = place.astype(jnp.float32) * freqs
    sine = jnp.sin(angle)
    return jnp.cos(angle), jnp.where(lane % (2 * quarter) < quarter, -sine, sine)


def turner(head_dim):
    lane = lax.broadcasted_iota(jnp.int32, (1, LANES), 1)
    first = lane % (head_dim // 2) < head_dim // 4
    a = lax.broadcasted_iota(jnp.int32, (LANES, LANES), 0) // head_dim
    b = lax.broadcasted_iota(jnp.int32, (LANES, LANES), 1) // head_dim
    average = jnp.where(a == b, 1.0 / head_dim, 0.0).astype(jnp.float32)

    def scaled(values, gains):
        mean_sq = jnp.dot(
            values * values,
            average,
            preferred_element_type=jnp.float32,
            precision=lax.Precision.HIGHEST,
        )
        return values * lax.rsqrt(mean_sq + epsilon) * gains

    def turned(values, cosine, sine):
        ahead = pltpu.roll(values, LANES - head_dim // 4, 1)
        behind = pltpu.roll(values, head_dim // 4, 1)
        return values * cosine + jnp.where(first, ahead, behind) * sine

    return scaled, turned, lane < head_dim


def contract_last(a, b):
    return lax.dot_general(a, b, (((1,), (1,)), ((), ())), preferred_element_type=jnp.float32)


def start_all(pairs, sems):
    copies = [pltpu.make_async_copy(a, b, sems.at[i]) for i, (a, b) in enumerate(pairs)]
    for copy in copies:
        copy.start()
    return copies


def modulate(cond_ref, w_hbm, out_ref, w_ref, sems):
    (copy,) = start_all(((w_hbm, w_ref),), sems)
    cond = cond_ref[...].astype(jnp.float32)
    active = (cond / (1.0 + jnp.exp(-cond))).astype(jnp.bfloat16)
    active = jnp.broadcast_to(active, (16, active.shape[1]))
    copy.wait()
    piece = contract_last(active, w_ref[...])[0:1]
    out_ref[...] = jnp.broadcast_to(piece[None], out_ref.shape)


def prepare(
    lat_hbm, ctx_hbm, wk_hbm, wv_hbm, kg_ref, inv_ref, ctx_kv_ref, lat_ref, ctx_ref, wkv_ref, sems
):
    rows = lat_ref.shape[0]
    head_dim = kg_ref.shape[1]
    copies = start_all(
        (
            (lat_hbm, lat_ref),
            (ctx_hbm, ctx_ref),
            (wk_hbm, wkv_ref.at[pl.ds(0, head_dim)]),
            (wv_hbm, wkv_ref.at[pl.ds(head_dim, head_dim)]),
        ),
        sems,
    )
    copies[0].wait()
    step = 32
    for r in range(0, rows, step):
        x = lat_ref[r : r + step, :].astype(jnp.float32)
        mean_sq = jnp.mean(x * x, axis=-1, keepdims=True)
        inv_ref[r : r + step, :] = jnp.broadcast_to(lax.rsqrt(mean_sq + epsilon), (step, LANES))
    for copy in copies[1:]:
        copy.wait()
    scaled, _, low = turner(head_dim)
    both = contract_last(ctx_ref[...], wkv_ref[...])
    kg = jnp.concatenate([kg_ref[...]] * 2, axis=1)
    ctx_kv_ref[...] = jnp.where(low, scaled(both, kg), both).astype(jnp.bfloat16)


def project(
    lat_hbm,
    wq_hbm,
    wk_hbm,
    wv_hbm,
    inv_ref,
    ctx_kv_ref,
    mod_ref,
    gain_ref,
    qg_ref,
    kg_ref,
    cos_ref,
    sin_ref,
    q_hbm,
    main_hbm,
    rest_hbm,
    gate_ref,
    lat_ref,
    wq_ref,
    wkv_ref,
    hid_ref,
    mods_ref,
    q_ref,
    kv_ref,
    sems,
    out_sems,
):
    rows, width = lat_ref.shape
    main = main_hbm.shape[0]
    rest = rest_hbm.shape[1]
    head_dim = qg_ref.shape[1]
    copies = start_all(
        (
            (lat_hbm, lat_ref),
            (wk_hbm, wkv_ref.at[pl.ds(0, head_dim)]),
            (wv_hbm, wkv_ref.at[pl.ds(head_dim, head_dim)]),
            (wq_hbm, wq_ref),
        ),
        sems,
    )
    pieces, _, piece = mod_ref.shape
    for j in range(pieces):
        mods_ref[0:1, piece * j : piece * (j + 1)] = mod_ref[j]
    shift = mods_ref[0:1, 0:width]
    scale = 1.0 + mods_ref[0:1, width : 2 * width]
    gate_ref[...] = mods_ref[0:1, 2 * width : 3 * width]
    gain = gain_ref[...]
    step = 32
    copies[0].wait()
    for r in range(0, rows, step):
        x = lat_ref[r : r + step, :].astype(jnp.float32)
        hidden = x * inv_ref[r : r + step, 0:1] * gain * scale + shift
        hid_ref[r : r + step, :] = hidden.astype(jnp.bfloat16)

    scaled, turned, low = turner(head_dim)
    qg = jnp.concatenate([qg_ref[...]] * 2, axis=1)
    kg = jnp.concatenate([kg_ref[...]] * 2, axis=1)
    cosine, sine = cos_ref[...], sin_ref[...]
    hid = hid_ref[...]
    copies[1].wait()
    copies[2].wait()
    both = contract_last(hid, wkv_ref[...])
    both = jnp.where(low, turned(scaled(both, kg), cosine, sine), both).astype(jnp.bfloat16)
    kv_ref[0:rows, :] = both
    kv_ref[rows:, :] = ctx_kv_ref[...]
    sent = kv_ref.at[pl.ds(main, rest)]
    outs = start_all(
        [(kv_ref.at[pl.ds(0, main)], main_hbm)]
        + [(sent, rest_hbm.at[z]) for z in range(rest_hbm.shape[0])],
        out_sems,
    )
    copies[3].wait()
    queries = jnp.dot(hid, wq_ref[...], preferred_element_type=jnp.float32)
    for g in range(queries.shape[1] // LANES):
        pair = turned(scaled(queries[:, LANES * g : LANES * (g + 1)], qg), cosine, sine)
        pair = pair.astype(jnp.bfloat16).astype(jnp.float32) * head_dim**-0.5
        other = pltpu.roll(pair, head_dim, 1)
        q_ref[2 * g] = jnp.where(low, pair, 0.0).astype(jnp.bfloat16)
        q_ref[2 * g + 1] = jnp.where(low, other, 0.0).astype(jnp.bfloat16)
    last = pltpu.make_async_copy(q_ref, q_hbm, sems.at[4])
    last.start()
    for copy in outs:
        copy.wait()
    last.wait()


def attend(q_hbm, main_ref, rest_ref, at_ref, q_ref, s_ref, sems):
    copies = start_all(((q_hbm, q_ref),), sems)
    heads, rows, _ = q_ref.shape
    head_dim = at_ref.shape[1] // heads
    parts, at = [], 0
    for ref in (main_ref, rest_ref):
        count = ref.shape[0]
        for c in range(0, count, KEY_STEP):
            size = min(KEY_STEP, count - c)
            parts.append((ref, c, at, size))
            at += size
    copies[0].wait()
    row_max = None
    for h in range(heads + 1):
        if h < heads:
            q = q_ref[h]
            m = jnp.full((rows, LANES), -jnp.inf, jnp.float32)
        if h > 0:
            total = jnp.zeros((rows, LANES), jnp.float32)
            acc = jnp.zeros((rows, LANES), jnp.float32)
        for ref, c, at, size in parts:
            if h < heads:
                s = contract_last(q, ref[c : c + size, :])
                s_ref[h % 2, :, at : at + size] = s
                for j in range(0, size, LANES):
                    m = jnp.maximum(m, s[:, j : j + LANES])
            if h > 0:
                p = jnp.exp(s_ref[(h + 1) % 2, :, at : at + size] - row_max)
                for j in range(0, size, LANES):
                    total = total + p[:, j : j + LANES]
                acc = acc + jnp.dot(
                    p.astype(jnp.bfloat16), ref[c : c + size, :], preferred_element_type=jnp.float32
                )
        if h > 0:
            total = jnp.sum(total, axis=1, keepdims=True)
            at_ref[:, head_dim * (h - 1) : head_dim * h] = (acc[:, head_dim:] / total).astype(
                jnp.bfloat16
            )
        row_max = jnp.max(m, axis=1, keepdims=True)


def finish(at_ref, lat_hbm, *refs):
    group = len(refs) - 6
    weights_hbm, (att_ref, gate_ref, out_ref, kept_ref, w_ref, sems) = refs[:group], refs[group:]
    kept = kept_ref.shape[0]
    own = at_ref[0]
    at = pl.multiple_of(own * kept, kept)
    copies = start_all(
        [(w, w_ref.at[k]) for k, w in enumerate(weights_hbm)]
        + [(lat_hbm.at[pl.ds(at, kept)], kept_ref)],
        sems,
    )
    projected = None
    for k in range(group):
        copies[k].wait()
        heads = att_ref[(own + group - k) % group]
        term = jnp.dot(heads, w_ref[k], preferred_element_type=jnp.float32)
        term = term.astype(jnp.bfloat16).astype(jnp.float32)
        projected = term if projected is None else projected + term
    copies[group].wait()
    residual = kept_ref[...].astype(jnp.float32)
    out_ref[...] = (residual + gate_ref[...] * projected).astype(jnp.bfloat16)


def vmem(mebibytes):
    return pltpu.CompilerParams(vmem_limit_bytes=mebibytes * 2**20)


def in_vmem(count):
    return [pl.BlockSpec(memory_space=pltpu.VMEM)] * count


def in_hbm(count):
    return [pl.BlockSpec(memory_space=pltpu.HBM)] * count


def one_device(
    latent,
    context,
    condition,
    mod_weight,
    norm_gain,
    w_query,
    w_key,
    w_value,
    q_gain,
    k_gain,
    w_out,
):
    _, length, width = latent.shape
    count = context.shape[1]
    head_dim = q_gain.shape[0]
    heads = w_query.shape[1] // head_dim
    sp, tp = lax.axis_size("sp"), lax.axis_size("tp")
    kept = length // tp
    main = length - 8
    rest = length - main + count
    half, single = jnp.bfloat16, jnp.float32
    shape = jax.ShapeDtypeStruct
    dma = lambda count: pltpu.SemaphoreType.DMA((count,))
    mod_pieces = pl.pallas_call(
        modulate,
        out_shape=shape((sp * tp, 1, mod_weight.shape[1]), single),
        in_specs=in_vmem(1) + in_hbm(1),
        scratch_shapes=[pltpu.VMEM(mod_weight.shape[::-1], half), dma(1)],
        compiler_params=vmem(8),
        name="modulate",
    )(condition, mod_weight.T)
    modulation = lax.all_to_all(mod_pieces, ("sp", "tp"), 0, 0, tiled=True)
    others = []
    for k in range(1, tp):
        others.append(lax.ppermute(w_out, "tp", [(i, (i + k) % tp) for i in range(tp)]))
    cosine, sine = rotary_tables(lax.axis_index("sp") * length, length, 0, head_dim)

    wk, wv = w_key.T, w_value.T
    inverse, ctx_kv = pl.pallas_call(
        prepare,
        out_shape=(shape((length, LANES), single), shape((count, LANES), half)),
        in_specs=in_hbm(4) + in_vmem(1),
        scratch_shapes=[
            pltpu.VMEM((length, width), half),
            pltpu.VMEM((count, width), half),
            pltpu.VMEM((2 * head_dim, width), half),
            dma(4),
        ],
        compiler_params=vmem(12),
        name="prepare",
    )(latent[0], context[0], wk, wv, k_gain[None])
    queries, own_main, own_rest, gate = pl.pallas_call(
        project,
        out_shape=(
            shape((heads, length, LANES), half),
            shape((main, LANES), half),
            shape((sp, rest, LANES), half),
            shape((1, width), single),
        ),
        in_specs=in_hbm(4) + in_vmem(8),
        out_specs=tuple(in_hbm(3) + in_vmem(1)),
        scratch_shapes=[
            pltpu.VMEM((length, width), half),
            pltpu.VMEM(w_query.shape, half),
            pltpu.VMEM((2 * head_dim, width), half),
            pltpu.VMEM((length, width), half),
            pltpu.VMEM((8, 3 * width), single),
            pltpu.VMEM((heads, length, LANES), half),
            pltpu.VMEM((main + rest, LANES), half),
            dma(5),
            dma(1 + sp),
        ],
        compiler_params=vmem(60),
        name="project",
    )(
        latent[0],
        w_query,
        wk,
        wv,
        inverse,
        ctx_kv,
        modulation,
        norm_gain[None],
        q_gain[None],
        k_gain[None],
        cosine,
        sine,
    )
    all_rest = lax.all_to_all(own_rest, "sp", 0, 0, tiled=True).reshape(sp * rest, LANES)
    all_main = lax.all_gather(own_main, "sp", axis=0, tiled=True)
    all_keys = sp * (main + rest)
    attended = pl.pallas_call(
        attend,
        out_shape=shape((length, heads * head_dim), half),
        in_specs=in_hbm(1) + in_vmem(2),
        scratch_shapes=[
            pltpu.VMEM((heads, length, LANES), half),
            pltpu.VMEM((2, length, all_keys), single),
            dma(1),
        ],
        compiler_params=vmem(32),
        name="attend",
    )(queries, all_main, all_rest)
    attended = attended.reshape(tp, kept, heads * head_dim)
    attended = lax.all_to_all(attended, "tp", 0, 0, tiled=True)
    mixed = pl.pallas_call(
        finish,
        out_shape=shape((kept, width), half),
        in_specs=[pl.BlockSpec(memory_space=pltpu.SMEM)] + in_hbm(1 + tp) + in_vmem(2),
        scratch_shapes=[
            pltpu.VMEM((kept, width), half),
            pltpu.VMEM((tp, *w_out.shape), half),
            dma(1 + tp),
        ],
        compiler_params=vmem(16),
        name="finish",
    )(
        lax.axis_index("tp").astype(jnp.int32)[None],
        latent[0],
        w_out,
        *others,
        attended,
        gate,
    )
    return mixed[None]


def solution(mesh):
    placed = (
        P("dp", "sp", None),
        P("dp", "sp", None),
        P("dp", None),
        P(None, ("sp", "tp")),
        P(),
        P(None, "tp"),
        P(None, "tp"),
        P(None, "tp"),
        P(),
        P(),
        P("tp", None),
    )
    return jax.shard_map(
        one_device, mesh=mesh, in_specs=placed, out_specs=P("dp", ("sp", "tp"), None), check_vma=False
    )
```

```python
import jax
import jax.numpy as jnp
from jax import lax
from jax.experimental import pallas as pl
from jax.experimental.pallas import tpu as pltpu
from jax.sharding import PartitionSpec as P

GRID_W = 64
LANES = 128
KEY_STEP = 512

epsilon = 1e-06
rope_base = 10000.0


def rotary_tables(first, rows, extra, head_dim):
    shape = (rows + extra, LANES)
    row = lax.broadcasted_iota(jnp.int32, shape, 0)
    lane = lax.broadcasted_iota(jnp.int32, shape, 1)
    where = first + row
    quarter = head_dim // 4
    place = jnp.where(lane % head_dim < head_dim // 2, where // GRID_W, where % GRID_W)
    place = jnp.where(row < rows, place, 0)
    freqs = rope_base ** (-(lane % quarter).astype(jnp.float32) / quarter)
    angle = place.astype(jnp.float32) * freqs
    sine = jnp.sin(angle)
    return jnp.cos(angle), jnp.where(lane % (2 * quarter) < quarter, -sine, sine)


def turner(head_dim):
    lane = lax.broadcasted_iota(jnp.int32, (1, LANES), 1)
    first = lane % (head_dim // 2) < head_dim // 4
    a = lax.broadcasted_iota(jnp.int32, (LANES, LANES), 0) // head_dim
    b = lax.broadcasted_iota(jnp.int32, (LANES, LANES), 1) // head_dim
    average = jnp.where(a == b, 1.0 / head_dim, 0.0).astype(jnp.float32)

    def scaled(values, gains):
        mean_sq = jnp.dot(
            values * values,
            average,
            preferred_element_type=jnp.float32,
            precision=lax.Precision.HIGHEST,
        )
        return values * lax.rsqrt(mean_sq + epsilon) * gains

    def turned(values, cosine, sine):
        ahead = pltpu.roll(values, LANES - head_dim // 4, 1)
        behind = pltpu.roll(values, head_dim // 4, 1)
        return values * cosine + jnp.where(first, ahead, behind) * sine

    return scaled, turned, lane < head_dim


def contract_last(a, b):
    return lax.dot_general(a, b, (((1,), (1,)), ((), ())), preferred_element_type=jnp.float32)


def start_all(pairs, sems):
    copies = [pltpu.make_async_copy(a, b, sems.at[i]) for i, (a, b) in enumerate(pairs)]
    for copy in copies:
        copy.start()
    return copies


def modulate(cond_ref, w_hbm, out_ref, w_ref, sems):
    (copy,) = start_all(((w_hbm, w_ref),), sems)
    cond = cond_ref[...].astype(jnp.float32)
    active = (cond / (1.0 + jnp.exp(-cond))).astype(jnp.bfloat16)
    active = jnp.broadcast_to(active, (16, active.shape[1]))
    copy.wait()
    piece = contract_last(active, w_ref[...])[0:1]
    out_ref[...] = jnp.broadcast_to(piece[None], out_ref.shape)


def prepare(
    lat_ref, ctx_ref, wk_ref, wv_ref, kg_ref, inv_ref, ctx_kv_ref, wkv_ref
):
    rows = lat_ref.shape[0]
    head_dim = kg_ref.shape[1]
    step = 32
    for r in range(0, rows, step):
        x = lat_ref[r : r + step, :].astype(jnp.float32)
        mean_sq = jnp.mean(x * x, axis=-1, keepdims=True)
        inv_ref[r : r + step, :] = jnp.broadcast_to(lax.rsqrt(mean_sq + epsilon), (step, LANES))
    wkv_ref[0:head_dim, :] = wk_ref[...]
    wkv_ref[head_dim:, :] = wv_ref[...]
    scaled, _, low = turner(head_dim)
    both = contract_last(ctx_ref[...], wkv_ref[...])
    kg = jnp.concatenate([kg_ref[...]] * 2, axis=1)
    ctx_kv_ref[...] = jnp.where(low, scaled(both, kg), both).astype(jnp.bfloat16)


def project(
    lat_ref,
    wq_hbm,
    wkv_ref,
    inv_ref,
    ctx_kv_ref,
    mod_ref,
    gain_ref,
    qg_ref,
    kg_ref,
    cos_ref,
    sin_ref,
    q_hbm,
    main_hbm,
    rest_hbm,
    gate_ref,
    hid_ref,
    mods_ref,
    q_ref,
    kv_ref,
    wq_ref,
    wq_sems,
    q_sems,
    out_sems,
):
    (weights_in,) = start_all(((wq_hbm, wq_ref),), wq_sems)
    rows, width = lat_ref.shape
    main = main_hbm.shape[0]
    rest = rest_hbm.shape[1]
    head_dim = qg_ref.shape[1]
    pieces, _, piece = mod_ref.shape
    for j in range(pieces):
        mods_ref[0:1, piece * j : piece * (j + 1)] = mod_ref[j]
    shift = mods_ref[0:1, 0:width]
    scale = 1.0 + mods_ref[0:1, width : 2 * width]
    gate_ref[...] = mods_ref[0:1, 2 * width : 3 * width]
    gain = gain_ref[...]
    step = 32
    for r in range(0, rows, step):
        x = lat_ref[r : r + step, :].astype(jnp.float32)
        hidden = x * inv_ref[r : r + step, 0:1] * gain * scale + shift
        hid_ref[r : r + step, :] = hidden.astype(jnp.bfloat16)

    scaled, turned, low = turner(head_dim)
    qg = jnp.concatenate([qg_ref[...]] * 2, axis=1)
    kg = jnp.concatenate([kg_ref[...]] * 2, axis=1)
    cosine, sine = cos_ref[...], sin_ref[...]
    hid = hid_ref[...]
    both = contract_last(hid, wkv_ref[...])
    both = jnp.where(low, turned(scaled(both, kg), cosine, sine), both).astype(jnp.bfloat16)
    kv_ref[0:rows, :] = both
    kv_ref[rows:, :] = ctx_kv_ref[...]
    sent = kv_ref.at[pl.ds(main, rest)]
    outs = start_all(
        [(kv_ref.at[pl.ds(0, main)], main_hbm)]
        + [(sent, rest_hbm.at[z]) for z in range(rest_hbm.shape[0])],
        out_sems,
    )
    weights_in.wait()
    queries = jnp.dot(hid, wq_ref[...], preferred_element_type=jnp.float32)
    for g in range(queries.shape[1] // LANES):
        pair = turned(scaled(queries[:, LANES * g : LANES * (g + 1)], qg), cosine, sine)
        pair = pair.astype(jnp.bfloat16).astype(jnp.float32) * head_dim**-0.5
        other = pltpu.roll(pair, head_dim, 1)
        q_ref[2 * g] = jnp.where(low, pair, 0.0).astype(jnp.bfloat16)
        q_ref[2 * g + 1] = jnp.where(low, other, 0.0).astype(jnp.bfloat16)
        pair_of = pl.ds(2 * g, 2)
        outs += start_all(((q_ref.at[pair_of], q_hbm.at[pair_of]),), q_sems.at[pl.ds(g, 1)])
    for copy in outs:
        copy.wait()


def attend(q_hbm, main_ref, rest_ref, w_hbm, o_ref, q_ref, s_ref, at_ref, w_ref, sems):
    copies = start_all(((q_hbm, q_ref), (w_hbm, w_ref)), sems)
    heads, rows, _ = q_ref.shape
    head_dim = at_ref.shape[1] // heads
    parts, at = [], 0
    for ref in (main_ref, rest_ref):
        count = ref.shape[0]
        for c in range(0, count, KEY_STEP):
            size = min(KEY_STEP, count - c)
            parts.append((ref, c, at, size))
            at += size
    copies[0].wait()
    row_max = None
    for h in range(heads + 1):
        if h < heads:
            q = q_ref[h]
            m = jnp.full((rows, LANES), -jnp.inf, jnp.float32)
        if h > 0:
            total = jnp.zeros((rows, LANES), jnp.float32)
            acc = jnp.zeros((rows, LANES), jnp.float32)
        for ref, c, at, size in parts:
            if h < heads:
                s = contract_last(q, ref[c : c + size, :])
                s_ref[h % 2, :, at : at + size] = s
                for j in range(0, size, LANES):
                    m = jnp.maximum(m, s[:, j : j + LANES])
            if h > 0:
                p = jnp.exp(s_ref[(h + 1) % 2, :, at : at + size] - row_max)
                for j in range(0, size, LANES):
                    total = total + p[:, j : j + LANES]
                acc = acc + jnp.dot(
                    p.astype(jnp.bfloat16), ref[c : c + size, :], preferred_element_type=jnp.float32
                )
        if h > 0:
            total = jnp.sum(total, axis=1, keepdims=True)
            at_ref[:, head_dim * (h - 1) : head_dim * h] = (acc[:, head_dim:] / total).astype(
                jnp.bfloat16
            )
        row_max = jnp.max(m, axis=1, keepdims=True)
    copies[1].wait()
    o_ref[...] = jnp.dot(at_ref[...], w_ref[...], preferred_element_type=jnp.float32).astype(
        jnp.bfloat16
    )


def finish(at_ref, lat_hbm, terms_ref, gate_ref, out_ref, kept_ref, sems):
    kept = kept_ref.shape[0]
    at = pl.multiple_of(at_ref[0] * kept, kept)
    (copy,) = start_all(((lat_hbm.at[pl.ds(at, kept)], kept_ref),), sems)
    projected = terms_ref[0].astype(jnp.float32)
    for g in range(1, terms_ref.shape[0]):
        projected = projected + terms_ref[g].astype(jnp.float32)
    copy.wait()
    residual = kept_ref[...].astype(jnp.float32)
    out_ref[...] = (residual + gate_ref[...] * projected).astype(jnp.bfloat16)


def vmem(mebibytes):
    return pltpu.CompilerParams(vmem_limit_bytes=mebibytes * 2**20)


def in_vmem(count):
    return [pl.BlockSpec(memory_space=pltpu.VMEM)] * count


def in_hbm(count):
    return [pl.BlockSpec(memory_space=pltpu.HBM)] * count


def shards(
    latent,
    context,
    condition,
    mod_weight,
    norm_gain,
    w_query,
    w_key,
    w_value,
    q_gain,
    k_gain,
    w_out,
):
    _, length, width = latent.shape
    count = context.shape[1]
    head_dim = q_gain.shape[0]
    heads = w_query.shape[1] // head_dim
    sp, tp = lax.axis_size("sp"), lax.axis_size("tp")
    kept = length // tp
    main = length - 8
    rest = length - main + count
    half, single = jnp.bfloat16, jnp.float32
    shape = jax.ShapeDtypeStruct
    dma = lambda count: pltpu.SemaphoreType.DMA((count,))
    mod_pieces = pl.pallas_call(
        modulate,
        out_shape=shape((sp * tp, 1, mod_weight.shape[1]), single),
        in_specs=in_vmem(1) + in_hbm(1),
        scratch_shapes=[pltpu.VMEM(mod_weight.shape[::-1], half), dma(1)],
        compiler_params=vmem(60),
        name="modulate",
    )(condition, mod_weight.T)
    modulation = lax.all_to_all(mod_pieces, ("sp", "tp"), 0, 0, tiled=True)
    cosine, sine = rotary_tables(lax.axis_index("sp") * length, length, 0, head_dim)

    wk, wv = w_key.T, w_value.T
    inverse, ctx_kv, wkv = pl.pallas_call(
        prepare,
        out_shape=(
            shape((length, LANES), single),
            shape((count, LANES), half),
            shape((2 * head_dim, width), half),
        ),
        in_specs=in_vmem(5),
        compiler_params=vmem(8),
        name="prepare",
    )(latent[0], context[0], wk, wv, k_gain[None])
    queries, own_main, own_rest, gate = pl.pallas_call(
        project,
        out_shape=(
            shape((heads, length, LANES), half),
            shape((main, LANES), half),
            shape((sp, rest, LANES), half),
            shape((1, width), single),
        ),
        in_specs=in_vmem(1) + in_hbm(1) + in_vmem(9),
        out_specs=tuple(in_hbm(3) + in_vmem(1)),
        scratch_shapes=[
            pltpu.VMEM((length, width), half),
            pltpu.VMEM((8, 3 * width), single),
            pltpu.VMEM((heads, length, LANES), half),
            pltpu.VMEM((main + rest, LANES), half),
            pltpu.VMEM(w_query.shape, half),
            dma(1),
            dma(heads // 2),
            dma(1 + sp),
        ],
        compiler_params=vmem(16),
        name="project",
    )(
        latent[0],
        w_query,
        wkv,
        inverse,
        ctx_kv,
        modulation,
        norm_gain[None],
        q_gain[None],
        k_gain[None],
        cosine,
        sine,
    )
    all_rest = lax.all_to_all(own_rest, "sp", 0, 0, tiled=True).reshape(sp * rest, LANES)
    all_main = lax.all_gather(own_main, "sp", axis=0, tiled=True)
    all_keys = sp * (main + rest)
    terms = pl.pallas_call(
        attend,
        out_shape=shape((length, width), half),
        in_specs=in_hbm(1) + in_vmem(2) + in_hbm(1),
        scratch_shapes=[
            pltpu.VMEM((heads, length, LANES), half),
            pltpu.VMEM((2, length, all_keys), single),
            pltpu.VMEM((length, heads * head_dim), half),
            pltpu.VMEM(w_out.shape, half),
            dma(2),
        ],
        compiler_params=vmem(32),
        name="attend",
    )(queries, all_main, all_rest, w_out)
    terms = lax.all_to_all(terms.reshape(tp, kept, width), "tp", 0, 0, tiled=True)
    mixed = pl.pallas_call(
        finish,
        out_shape=shape((kept, width), half),
        in_specs=[pl.BlockSpec(memory_space=pltpu.SMEM)] + in_hbm(1) + in_vmem(2),
        scratch_shapes=[pltpu.VMEM((kept, width), half), dma(1)],
        compiler_params=vmem(8),
        name="finish",
    )(lax.axis_index("tp").astype(jnp.int32)[None], latent[0], terms, gate)
    return mixed[None]


def solution(mesh):
    placed = (
        P("dp", "sp", None),
        P("dp", "sp", None),
        P("dp", None),
        P(None, ("sp", "tp")),
        P(),
        P(None, "tp"),
        P(None, "tp"),
        P(None, "tp"),
        P(),
        P(),
        P("tp", None),
    )
    return jax.shard_map(
        shards, mesh=mesh, in_specs=placed, out_specs=P("dp", ("sp", "tp"), None), check_vma=False
    )
```

```python
import jax
import jax.numpy as jnp
from jax import lax
from jax.experimental import pallas as pl
from jax.experimental.pallas import tpu as pltpu
from jax.sharding import PartitionSpec as P

GRID_W = 64
LANES = 128
KEY_STEP = 512

epsilon = 1e-06
rope_base = 10000.0


def rotary_tables(first, rows, extra, head_dim):
    shape = (rows + extra, LANES)
    row = lax.broadcasted_iota(jnp.int32, shape, 0)
    lane = lax.broadcasted_iota(jnp.int32, shape, 1)
    where = first + row
    quarter = head_dim // 4
    place = jnp.where(lane % head_dim < head_dim // 2, where // GRID_W, where % GRID_W)
    place = jnp.where(row < rows, place, 0)
    freqs = rope_base ** (-(lane % quarter).astype(jnp.float32) / quarter)
    angle = place.astype(jnp.float32) * freqs
    sine = jnp.sin(angle)
    return jnp.cos(angle), jnp.where(lane % (2 * quarter) < quarter, -sine, sine)


def turner(head_dim):
    lane = lax.broadcasted_iota(jnp.int32, (1, LANES), 1)
    first = lane % (head_dim // 2) < head_dim // 4
    a = lax.broadcasted_iota(jnp.int32, (LANES, LANES), 0) // head_dim
    b = lax.broadcasted_iota(jnp.int32, (LANES, LANES), 1) // head_dim
    average = jnp.where(a == b, 1.0 / head_dim, 0.0).astype(jnp.float32)

    def scaled(values, gains):
        mean_sq = jnp.dot(
            values * values,
            average,
            preferred_element_type=jnp.float32,
            precision=lax.Precision.HIGHEST,
        )
        return values * lax.rsqrt(mean_sq + epsilon) * gains

    def turned(values, cosine, sine):
        ahead = pltpu.roll(values, LANES - head_dim // 4, 1)
        behind = pltpu.roll(values, head_dim // 4, 1)
        return values * cosine + jnp.where(first, ahead, behind) * sine

    return scaled, turned, lane < head_dim


def contract_last(a, b):
    return lax.dot_general(a, b, (((1,), (1,)), ((), ())), preferred_element_type=jnp.float32)


def start_all(pairs, sems):
    copies = [pltpu.make_async_copy(a, b, sems.at[i]) for i, (a, b) in enumerate(pairs)]
    for copy in copies:
        copy.start()
    return copies


def modulate(cond_hbm, w_hbm, out_ref, cond_ref, w_ref, sems):
    cond_in, copy = start_all(((cond_hbm, cond_ref), (w_hbm, w_ref)), sems)
    cond_in.wait()
    cond = cond_ref[...].astype(jnp.float32)
    active = (cond / (1.0 + jnp.exp(-cond))).astype(jnp.bfloat16)
    active = jnp.broadcast_to(active, (16, active.shape[1]))
    copy.wait()
    piece = contract_last(active, w_ref[...])[0:1]
    out_ref[...] = jnp.broadcast_to(piece[None], out_ref.shape)


def prepare(
    lat_hbm,
    ctx_hbm,
    wk_hbm,
    wv_hbm,
    qg_ref,
    kg_ref,
    inv_ref,
    ctx_kv_ref,
    wkv_ref,
    gains_ref,
    lat_ref,
    ctx_ref,
    sems,
):
    rows = lat_ref.shape[0]
    head_dim = kg_ref.shape[1]
    copies = start_all(
        (
            (lat_hbm, lat_ref),
            (ctx_hbm, ctx_ref),
            (wk_hbm, wkv_ref.at[pl.ds(0, head_dim)]),
            (wv_hbm, wkv_ref.at[pl.ds(head_dim, head_dim)]),
        ),
        sems,
    )
    kg = jnp.concatenate([kg_ref[...]] * 2, axis=1)
    gains_ref[0:1, :] = jnp.concatenate([qg_ref[...]] * 2, axis=1)
    gains_ref[1:2, :] = kg
    copies[0].wait()
    step = 32
    for r in range(0, rows, step):
        x = lat_ref[r : r + step, :].astype(jnp.float32)
        mean_sq = jnp.mean(x * x, axis=-1, keepdims=True)
        inv_ref[r : r + step, :] = jnp.broadcast_to(lax.rsqrt(mean_sq + epsilon), (step, LANES))
    for copy in copies[1:]:
        copy.wait()
    scaled, _, low = turner(head_dim)
    both = contract_last(ctx_ref[...], wkv_ref[...])
    ctx_kv_ref[...] = jnp.where(low, scaled(both, kg), both).astype(jnp.bfloat16)


def project(
    lat_ref,
    wq_ref,
    wkv_ref,
    inv_ref,
    ctx_kv_ref,
    mod_ref,
    gain_ref,
    gains_ref,
    cos_ref,
    sin_ref,
    q_hbm,
    main_hbm,
    rest_hbm,
    gate_ref,
    hid_ref,
    mods_ref,
    q_ref,
    kv_ref,
    q_sems,
    out_sems,
):
    rows, width = lat_ref.shape
    main = main_hbm.shape[0]
    rest = rest_hbm.shape[1]
    head_dim = wkv_ref.shape[0] // 2
    pieces, _, piece = mod_ref.shape
    for j in range(pieces):
        mods_ref[0:1, piece * j : piece * (j + 1)] = mod_ref[j]
    shift = mods_ref[0:1, 0:width]
    scale = 1.0 + mods_ref[0:1, width : 2 * width]
    gate_ref[...] = mods_ref[0:1, 2 * width : 3 * width]
    gain = gain_ref[...]
    step = 32
    for r in range(0, rows, step):
        x = lat_ref[r : r + step, :].astype(jnp.float32)
        hidden = x * inv_ref[r : r + step, 0:1] * gain * scale + shift
        hid_ref[r : r + step, :] = hidden.astype(jnp.bfloat16)

    scaled, turned, low = turner(head_dim)
    qg, kg = gains_ref[0:1, :], gains_ref[1:2, :]
    cosine, sine = cos_ref[...], sin_ref[...]
    hid = hid_ref[...]
    both = contract_last(hid, wkv_ref[...])
    both = jnp.where(low, turned(scaled(both, kg), cosine, sine), both).astype(jnp.bfloat16)
    kv_ref[0:rows, :] = both
    kv_ref[rows:, :] = ctx_kv_ref[...]
    sent = kv_ref.at[pl.ds(main, rest)]
    outs = start_all(
        [(kv_ref.at[pl.ds(0, main)], main_hbm)]
        + [(sent, rest_hbm.at[z]) for z in range(rest_hbm.shape[0])],
        out_sems,
    )
    queries = jnp.dot(hid, wq_ref[...], preferred_element_type=jnp.float32)
    for g in range(queries.shape[1] // LANES):
        pair = turned(scaled(queries[:, LANES * g : LANES * (g + 1)], qg), cosine, sine)
        pair = pair.astype(jnp.bfloat16).astype(jnp.float32) * head_dim**-0.5
        other = pltpu.roll(pair, head_dim, 1)
        q_ref[2 * g] = jnp.where(low, pair, 0.0).astype(jnp.bfloat16)
        q_ref[2 * g + 1] = jnp.where(low, other, 0.0).astype(jnp.bfloat16)
        pair_of = pl.ds(2 * g, 2)
        outs += start_all(((q_ref.at[pair_of], q_hbm.at[pair_of]),), q_sems.at[pl.ds(g, 1)])
    for copy in outs:
        copy.wait()


def attend(q_ref, main_ref, rest_ref, w_hbm, o_ref, s_ref, at_ref, w_ref, sems):
    (weights_in,) = start_all(((w_hbm, w_ref),), sems)
    heads, rows, _ = q_ref.shape
    head_dim = at_ref.shape[1] // heads
    parts, at = [], 0
    for ref in (main_ref, rest_ref):
        count = ref.shape[0]
        for c in range(0, count, KEY_STEP):
            size = min(KEY_STEP, count - c)
            parts.append((ref, c, at, size))
            at += size
    row_max = None
    for h in range(heads + 1):
        if h < heads:
            q = q_ref[h]
            m = jnp.full((rows, LANES), -jnp.inf, jnp.float32)
        if h > 0:
            total = jnp.zeros((rows, LANES), jnp.float32)
            acc = jnp.zeros((rows, LANES), jnp.float32)
        for ref, c, at, size in parts:
            if h < heads:
                s = contract_last(q, ref[c : c + size, :])
                s_ref[h % 2, :, at : at + size] = s
                for j in range(0, size, LANES):
                    m = jnp.maximum(m, s[:, j : j + LANES])
            if h > 0:
                p = jnp.exp(s_ref[(h + 1) % 2, :, at : at + size] - row_max)
                for j in range(0, size, LANES):
                    total = total + p[:, j : j + LANES]
                acc = acc + jnp.dot(
                    p.astype(jnp.bfloat16), ref[c : c + size, :], preferred_element_type=jnp.float32
                )
        if h > 0:
            total = jnp.sum(total, axis=1, keepdims=True)
            at_ref[:, head_dim * (h - 1) : head_dim * h] = (acc[:, head_dim:] / total).astype(
                jnp.bfloat16
            )
        row_max = jnp.max(m, axis=1, keepdims=True)
    weights_in.wait()
    o_ref[...] = jnp.dot(at_ref[...], w_ref[...], preferred_element_type=jnp.float32).astype(
        jnp.bfloat16
    )


def finish(at_ref, lat_hbm, terms_ref, gate_ref, out_ref, kept_ref, sems):
    kept = kept_ref.shape[0]
    at = pl.multiple_of(at_ref[0] * kept, kept)
    (copy,) = start_all(((lat_hbm.at[pl.ds(at, kept)], kept_ref),), sems)
    projected = terms_ref[0].astype(jnp.float32)
    for g in range(1, terms_ref.shape[0]):
        projected = projected + terms_ref[g].astype(jnp.float32)
    copy.wait()
    residual = kept_ref[...].astype(jnp.float32)
    out_ref[...] = (residual + gate_ref[...] * projected).astype(jnp.bfloat16)


def vmem(mebibytes):
    return pltpu.CompilerParams(vmem_limit_bytes=mebibytes * 2**20)


def in_vmem(count):
    return [pl.BlockSpec(memory_space=pltpu.VMEM)] * count


def in_hbm(count):
    return [pl.BlockSpec(memory_space=pltpu.HBM)] * count


def shards(
    latent,
    context,
    condition,
    mod_weight,
    norm_gain,
    w_query,
    w_key,
    w_value,
    q_gain,
    k_gain,
    w_out,
):
    _, length, width = latent.shape
    count = context.shape[1]
    head_dim = q_gain.shape[0]
    heads = w_query.shape[1] // head_dim
    sp, tp = lax.axis_size("sp"), lax.axis_size("tp")
    kept = length // tp
    main = length - 8
    rest = length - main + count
    half, single = jnp.bfloat16, jnp.float32
    shape = jax.ShapeDtypeStruct
    dma = lambda count: pltpu.SemaphoreType.DMA((count,))
    mod_pieces = pl.pallas_call(
        modulate,
        out_shape=shape((sp * tp, 1, mod_weight.shape[1]), single),
        in_specs=in_hbm(2),
        scratch_shapes=[
            pltpu.VMEM(condition.shape, half),
            pltpu.VMEM(mod_weight.shape[::-1], half),
            dma(2),
        ],
        compiler_params=vmem(60),
        name="modulate",
    )(condition, mod_weight.T)
    modulation = lax.all_to_all(mod_pieces, ("sp", "tp"), 0, 0, tiled=True)
    cosine, sine = rotary_tables(lax.axis_index("sp") * length, length, 0, head_dim)

    wk, wv = w_key.T, w_value.T
    inverse, ctx_kv, wkv, gains = pl.pallas_call(
        prepare,
        out_shape=(
            shape((length, LANES), single),
            shape((count, LANES), half),
            shape((2 * head_dim, width), half),
            shape((2, LANES), single),
        ),
        in_specs=in_hbm(4) + in_vmem(2),
        scratch_shapes=[pltpu.VMEM((length, width), half), pltpu.VMEM((count, width), half), dma(4)],
        compiler_params=vmem(52),
        name="prepare",
    )(latent[0], context[0], wk, wv, q_gain[None], k_gain[None])
    queries, own_main, own_rest, gate = pl.pallas_call(
        project,
        out_shape=(
            shape((heads, length, LANES), half),
            shape((main, LANES), half),
            shape((sp, rest, LANES), half),
            shape((1, width), single),
        ),
        in_specs=in_vmem(10),
        out_specs=tuple(in_hbm(3) + in_vmem(1)),
        scratch_shapes=[
            pltpu.VMEM((length, width), half),
            pltpu.VMEM((8, 3 * width), single),
            pltpu.VMEM((heads, length, LANES), half),
            pltpu.VMEM((main + rest, LANES), half),
            dma(heads // 2),
            dma(1 + sp),
        ],
        compiler_params=vmem(16),
        name="project",
    )(
        latent[0],
        w_query,
        wkv,
        inverse,
        ctx_kv,
        modulation,
        norm_gain[None],
        gains,
        cosine,
        sine,
    )
    all_rest = lax.all_to_all(own_rest, "sp", 0, 0, tiled=True).reshape(sp * rest, LANES)
    all_main = lax.all_gather(own_main, "sp", axis=0, tiled=True)
    all_keys = sp * (main + rest)
    terms = pl.pallas_call(
        attend,
        out_shape=shape((length, width), half),
        in_specs=in_vmem(3) + in_hbm(1),
        scratch_shapes=[
            pltpu.VMEM((2, length, all_keys), single),
            pltpu.VMEM((length, heads * head_dim), half),
            pltpu.VMEM(w_out.shape, half),
            dma(1),
        ],
        compiler_params=vmem(32),
        name="attend",
    )(queries, all_main, all_rest, w_out)
    terms = lax.all_to_all(terms.reshape(tp, kept, width), "tp", 0, 0, tiled=True)
    mixed = pl.pallas_call(
        finish,
        out_shape=shape((kept, width), half),
        in_specs=[pl.BlockSpec(memory_space=pltpu.SMEM)] + in_hbm(1) + in_vmem(2),
        scratch_shapes=[pltpu.VMEM((kept, width), half), dma(1)],
        compiler_params=vmem(8),
        name="finish",
    )(lax.axis_index("tp").astype(jnp.int32)[None], latent[0], terms, gate)
    return mixed[None]


def solution(mesh):
    placed = (
        P("dp", "sp", None),
        P("dp", "sp", None),
        P("dp", None),
        P(None, ("sp", "tp")),
        P(),
        P(None, "tp"),
        P(None, "tp"),
        P(None, "tp"),
        P(),
        P(),
        P("tp", None),
    )
    return jax.shard_map(
        shards, mesh=mesh, in_specs=placed, out_specs=P("dp", ("sp", "tp"), None), check_vma=False
    )
```

```python
import jax
import jax.numpy as jnp
from jax import lax
from jax.experimental import pallas as pl
from jax.experimental.pallas import tpu as pltpu
from jax.sharding import PartitionSpec as P

GRID_W = 64
LANES = 128
KEY_STEP = 512

epsilon = 1e-06
rope_base = 10000.0


def rotary_tables(first, rows, extra, head_dim):
    shape = (rows + extra, LANES)
    row = lax.broadcasted_iota(jnp.int32, shape, 0)
    lane = lax.broadcasted_iota(jnp.int32, shape, 1)
    where = first + row
    quarter = head_dim // 4
    place = jnp.where(lane % head_dim < head_dim // 2, where // GRID_W, where % GRID_W)
    place = jnp.where(row < rows, place, 0)
    freqs = rope_base ** (-(lane % quarter).astype(jnp.float32) / quarter)
    angle = place.astype(jnp.float32) * freqs
    sine = jnp.sin(angle)
    return jnp.cos(angle), jnp.where(lane % (2 * quarter) < quarter, -sine, sine)


def turner(head_dim):
    lane = lax.broadcasted_iota(jnp.int32, (1, LANES), 1)
    first = lane % (head_dim // 2) < head_dim // 4
    a = lax.broadcasted_iota(jnp.int32, (LANES, LANES), 0) // head_dim
    b = lax.broadcasted_iota(jnp.int32, (LANES, LANES), 1) // head_dim
    average = jnp.where(a == b, 1.0 / head_dim, 0.0).astype(jnp.float32)

    def scaled(values, gains):
        mean_sq = jnp.dot(
            values * values,
            average,
            preferred_element_type=jnp.float32,
            precision=lax.Precision.HIGHEST,
        )
        return values * lax.rsqrt(mean_sq + epsilon) * gains

    def turned(values, cosine, sine):
        ahead = pltpu.roll(values, LANES - head_dim // 4, 1)
        behind = pltpu.roll(values, head_dim // 4, 1)
        return values * cosine + jnp.where(first, ahead, behind) * sine

    return scaled, turned, lane < head_dim


def contract_last(a, b):
    return lax.dot_general(a, b, (((1,), (1,)), ((), ())), preferred_element_type=jnp.float32)


def start_all(pairs, sems):
    copies = [pltpu.make_async_copy(a, b, sems.at[i]) for i, (a, b) in enumerate(pairs)]
    for copy in copies:
        copy.start()
    return copies


def modulate(cond_hbm, w_hbm, out_ref, cond_ref, w_ref, sems):
    cond_in, copy = start_all(((cond_hbm, cond_ref), (w_hbm, w_ref)), sems)
    cond_in.wait()
    cond = cond_ref[...].astype(jnp.float32)
    active = (cond / (1.0 + jnp.exp(-cond))).astype(jnp.bfloat16)
    active = jnp.broadcast_to(active, (16, active.shape[1]))
    copy.wait()
    piece = contract_last(active, w_ref[...])[0:1]
    out_ref[...] = jnp.broadcast_to(piece[None], out_ref.shape)


def prepare(
    lat_hbm,
    ctx_hbm,
    wk_hbm,
    wv_hbm,
    qg_ref,
    kg_ref,
    inv_ref,
    ctx_kv_ref,
    wkv_ref,
    gains_ref,
    lat_ref,
    ctx_ref,
    sems,
):
    rows = lat_ref.shape[0]
    head_dim = kg_ref.shape[1]
    copies = start_all(
        (
            (lat_hbm, lat_ref),
            (ctx_hbm, ctx_ref),
            (wk_hbm, wkv_ref.at[pl.ds(0, head_dim)]),
            (wv_hbm, wkv_ref.at[pl.ds(head_dim, head_dim)]),
        ),
        sems,
    )
    kg = jnp.concatenate([kg_ref[...]] * 2, axis=1)
    gains_ref[0:1, :] = jnp.concatenate([qg_ref[...]] * 2, axis=1)
    gains_ref[1:2, :] = kg
    copies[0].wait()
    step = 32
    for r in range(0, rows, step):
        x = lat_ref[r : r + step, :].astype(jnp.float32)
        mean_sq = jnp.mean(x * x, axis=-1, keepdims=True)
        inv_ref[r : r + step, :] = jnp.broadcast_to(lax.rsqrt(mean_sq + epsilon), (step, LANES))
    for copy in copies[1:]:
        copy.wait()
    scaled, _, low = turner(head_dim)
    both = contract_last(ctx_ref[...], wkv_ref[...])
    ctx_kv_ref[...] = jnp.where(low, scaled(both, kg), both).astype(jnp.bfloat16)


def project(
    lat_ref,
    wq_ref,
    wkv_ref,
    inv_ref,
    ctx_kv_ref,
    mod_ref,
    gain_ref,
    gains_ref,
    cos_ref,
    sin_ref,
    q_hbm,
    main_hbm,
    rest_hbm,
    gate_ref,
    hid_ref,
    mods_ref,
    q_ref,
    kv_ref,
    q_sems,
    out_sems,
):
    rows, width = lat_ref.shape
    main = main_hbm.shape[0]
    rest = rest_hbm.shape[1]
    head_dim = wkv_ref.shape[0] // 2
    pieces, _, piece = mod_ref.shape
    for j in range(pieces):
        mods_ref[0:1, piece * j : piece * (j + 1)] = mod_ref[j]
    shift = mods_ref[0:1, 0:width]
    scale = 1.0 + mods_ref[0:1, width : 2 * width]
    gate_ref[...] = mods_ref[0:1, 2 * width : 3 * width]
    gain = gain_ref[...]
    step = 32
    for r in range(0, rows, step):
        x = lat_ref[r : r + step, :].astype(jnp.float32)
        hidden = x * inv_ref[r : r + step, 0:1] * gain * scale + shift
        hid_ref[r : r + step, :] = hidden.astype(jnp.bfloat16)

    scaled, turned, low = turner(head_dim)
    qg, kg = gains_ref[0:1, :], gains_ref[1:2, :]
    cosine, sine = cos_ref[...], sin_ref[...]
    hid = hid_ref[...]
    both = contract_last(hid, wkv_ref[...])
    both = jnp.where(low, turned(scaled(both, kg), cosine, sine), both).astype(jnp.bfloat16)
    kv_ref[0:rows, :] = both
    kv_ref[rows:, :] = ctx_kv_ref[...]
    sent = kv_ref.at[pl.ds(main, rest)]
    outs = start_all(
        [(kv_ref.at[pl.ds(0, main)], main_hbm)]
        + [(sent, rest_hbm.at[z]) for z in range(rest_hbm.shape[0])],
        out_sems,
    )
    queries = jnp.dot(hid, wq_ref[...], preferred_element_type=jnp.float32)
    for g in range(queries.shape[1] // LANES):
        pair = turned(scaled(queries[:, LANES * g : LANES * (g + 1)], qg), cosine, sine)
        pair = pair.astype(jnp.bfloat16).astype(jnp.float32) * head_dim**-0.5
        other = pltpu.roll(pair, head_dim, 1)
        q_ref[2 * g] = jnp.where(low, pair, 0.0).astype(jnp.bfloat16)
        q_ref[2 * g + 1] = jnp.where(low, other, 0.0).astype(jnp.bfloat16)
        pair_of = pl.ds(2 * g, 2)
        outs += start_all(((q_ref.at[pair_of], q_hbm.at[pair_of]),), q_sems.at[pl.ds(g, 1)])
    for copy in outs:
        copy.wait()


def attend(q_ref, main_ref, rest_ref, w_hbm, o_ref, s_ref, at_ref, w_ref, sems):
    (weights_in,) = start_all(((w_hbm, w_ref),), sems)
    heads, rows, _ = q_ref.shape
    head_dim = at_ref.shape[1] // heads
    parts, at = [], 0
    for ref in (main_ref, rest_ref):
        count = ref.shape[0]
        for c in range(0, count, KEY_STEP):
            size = min(KEY_STEP, count - c)
            parts.append((ref, c, at, size))
            at += size
    row_max = None
    for h in range(heads + 1):
        if h < heads:
            q = q_ref[h]
            m = jnp.full((rows, LANES), -jnp.inf, jnp.float32)
        if h > 0:
            total = jnp.zeros((rows, LANES), jnp.float32)
            acc = jnp.zeros((rows, LANES), jnp.float32)
        for ref, c, at, size in parts:
            if h < heads:
                s = contract_last(q, ref[c : c + size, :])
                s_ref[h % 2, :, at : at + size] = s
                for j in range(0, size, LANES):
                    m = jnp.maximum(m, s[:, j : j + LANES])
            if h > 0:
                p = jnp.exp(s_ref[(h + 1) % 2, :, at : at + size] - row_max)
                for j in range(0, size, LANES):
                    total = total + p[:, j : j + LANES]
                acc = acc + jnp.dot(
                    p.astype(jnp.bfloat16), ref[c : c + size, :], preferred_element_type=jnp.float32
                )
        if h > 0:
            total = jnp.sum(total, axis=1, keepdims=True)
            at_ref[:, head_dim * (h - 1) : head_dim * h] = (acc[:, head_dim:] / total).astype(
                jnp.bfloat16
            )
        row_max = jnp.max(m, axis=1, keepdims=True)
    weights_in.wait()
    o_ref[...] = jnp.dot(at_ref[...], w_ref[...], preferred_element_type=jnp.float32).astype(
        jnp.bfloat16
    )


def finish(lat_hbm, terms_ref, gate_ref, out_ref, kept_ref, sems):
    kept = kept_ref.shape[0]
    at = pl.multiple_of(lax.axis_index("tp") * kept, kept)
    (copy,) = start_all(((lat_hbm.at[pl.ds(at, kept)], kept_ref),), sems)
    projected = terms_ref[0].astype(jnp.float32)
    for g in range(1, terms_ref.shape[0]):
        projected = projected + terms_ref[g].astype(jnp.float32)
    copy.wait()
    residual = kept_ref[...].astype(jnp.float32)
    out_ref[...] = (residual + gate_ref[...] * projected).astype(jnp.bfloat16)


def vmem(mebibytes):
    return pltpu.CompilerParams(vmem_limit_bytes=mebibytes * 2**20)


def in_vmem(count):
    return [pl.BlockSpec(memory_space=pltpu.VMEM)] * count


def in_hbm(count):
    return [pl.BlockSpec(memory_space=pltpu.HBM)] * count


def shards(
    latent,
    context,
    condition,
    mod_weight,
    norm_gain,
    w_query,
    w_key,
    w_value,
    q_gain,
    k_gain,
    w_out,
):
    _, length, width = latent.shape
    count = context.shape[1]
    head_dim = q_gain.shape[0]
    heads = w_query.shape[1] // head_dim
    sp, tp = lax.axis_size("sp"), lax.axis_size("tp")
    kept = length // tp
    main = length - 8
    rest = length - main + count
    half, single = jnp.bfloat16, jnp.float32
    shape = jax.ShapeDtypeStruct
    dma = lambda count: pltpu.SemaphoreType.DMA((count,))
    mod_pieces = pl.pallas_call(
        modulate,
        out_shape=shape((sp * tp, 1, mod_weight.shape[1]), single),
        in_specs=in_hbm(2),
        scratch_shapes=[
            pltpu.VMEM(condition.shape, half),
            pltpu.VMEM(mod_weight.shape[::-1], half),
            dma(2),
        ],
        compiler_params=vmem(60),
        name="modulate",
    )(condition, mod_weight.T)
    modulation = lax.all_to_all(mod_pieces, ("sp", "tp"), 0, 0, tiled=True)
    cosine, sine = rotary_tables(lax.axis_index("sp") * length, length, 0, head_dim)

    wk, wv = w_key.T, w_value.T
    inverse, ctx_kv, wkv, gains = pl.pallas_call(
        prepare,
        out_shape=(
            shape((length, LANES), single),
            shape((count, LANES), half),
            shape((2 * head_dim, width), half),
            shape((2, LANES), single),
        ),
        in_specs=in_hbm(4) + in_vmem(2),
        scratch_shapes=[pltpu.VMEM((length, width), half), pltpu.VMEM((count, width), half), dma(4)],
        compiler_params=vmem(52),
        name="prepare",
    )(latent[0], context[0], wk, wv, q_gain[None], k_gain[None])
    queries, own_main, own_rest, gate = pl.pallas_call(
        project,
        out_shape=(
            shape((heads, length, LANES), half),
            shape((main, LANES), half),
            shape((sp, rest, LANES), half),
            shape((1, width), single),
        ),
        in_specs=in_vmem(10),
        out_specs=tuple(in_hbm(3) + in_vmem(1)),
        scratch_shapes=[
            pltpu.VMEM((length, width), half),
            pltpu.VMEM((8, 3 * width), single),
            pltpu.VMEM((heads, length, LANES), half),
            pltpu.VMEM((main + rest, LANES), half),
            dma(heads // 2),
            dma(1 + sp),
        ],
        compiler_params=vmem(16),
        name="project",
    )(
        latent[0],
        w_query,
        wkv,
        inverse,
        ctx_kv,
        modulation,
        norm_gain[None],
        gains,
        cosine,
        sine,
    )
    all_rest = lax.all_to_all(own_rest, "sp", 0, 0, tiled=True).reshape(sp * rest, LANES)
    all_main = lax.all_gather(own_main, "sp", axis=0, tiled=True)
    all_keys = sp * (main + rest)
    terms = pl.pallas_call(
        attend,
        out_shape=shape((length, width), half),
        in_specs=in_vmem(3) + in_hbm(1),
        scratch_shapes=[
            pltpu.VMEM((2, length, all_keys), single),
            pltpu.VMEM((length, heads * head_dim), half),
            pltpu.VMEM(w_out.shape, half),
            dma(1),
        ],
        compiler_params=vmem(32),
        name="attend",
    )(queries, all_main, all_rest, w_out)
    terms = lax.all_to_all(terms.reshape(tp, kept, width), "tp", 0, 0, tiled=True)
    mixed = pl.pallas_call(
        finish,
        out_shape=shape((kept, width), half),
        in_specs=in_hbm(1) + in_vmem(2),
        scratch_shapes=[pltpu.VMEM((kept, width), half), dma(1)],
        compiler_params=vmem(8),
        name="finish",
    )(latent[0], terms, gate)
    return mixed[None]


def solution(mesh):
    placed = (
        P("dp", "sp", None),
        P("dp", "sp", None),
        P("dp", None),
        P(None, ("sp", "tp")),
        P(),
        P(None, "tp"),
        P(None, "tp"),
        P(None, "tp"),
        P(),
        P(),
        P("tp", None),
    )
    return jax.shard_map(
        shards, mesh=mesh, in_specs=placed, out_specs=P("dp", ("sp", "tp"), None), check_vma=False
    )
```

```python
import jax
import jax.numpy as jnp
from jax import lax
from jax.experimental import pallas as pl
from jax.experimental.pallas import tpu as pltpu
from jax.sharding import PartitionSpec as P

GRID_W = 64
LANES = 128
KEY_STEP = 512

epsilon = 1e-06
rope_base = 10000.0


def rotary_tables(first, rows, extra, head_dim):
    shape = (rows + extra, LANES)
    row = lax.broadcasted_iota(jnp.int32, shape, 0)
    lane = lax.broadcasted_iota(jnp.int32, shape, 1)
    where = first + row
    quarter = head_dim // 4
    place = jnp.where(lane % head_dim < head_dim // 2, where // GRID_W, where % GRID_W)
    place = jnp.where(row < rows, place, 0)
    freqs = rope_base ** (-(lane % quarter).astype(jnp.float32) / quarter)
    angle = place.astype(jnp.float32) * freqs
    sine = jnp.sin(angle)
    return jnp.cos(angle), jnp.where(lane % (2 * quarter) < quarter, -sine, sine)


def turner(head_dim):
    lane = lax.broadcasted_iota(jnp.int32, (1, LANES), 1)
    first = lane % (head_dim // 2) < head_dim // 4
    a = lax.broadcasted_iota(jnp.int32, (LANES, LANES), 0) // head_dim
    b = lax.broadcasted_iota(jnp.int32, (LANES, LANES), 1) // head_dim
    average = jnp.where(a == b, 1.0 / head_dim, 0.0).astype(jnp.float32)

    def scaled(values, gains):
        mean_sq = jnp.dot(
            values * values,
            average,
            preferred_element_type=jnp.float32,
            precision=lax.Precision.HIGHEST,
        )
        return values * lax.rsqrt(mean_sq + epsilon) * gains

    def turned(values, cosine, sine):
        ahead = pltpu.roll(values, LANES - head_dim // 4, 1)
        behind = pltpu.roll(values, head_dim // 4, 1)
        return values * cosine + jnp.where(first, ahead, behind) * sine

    return scaled, turned, lane < head_dim


def contract_last(a, b):
    return lax.dot_general(a, b, (((1,), (1,)), ((), ())), preferred_element_type=jnp.float32)


def start_all(pairs, sems):
    copies = [pltpu.make_async_copy(a, b, sems.at[i]) for i, (a, b) in enumerate(pairs)]
    for copy in copies:
        copy.start()
    return copies


def modulate(cond_hbm, w_hbm, out_ref, cond_ref, w_ref, sems):
    cond_in, copy = start_all(((cond_hbm, cond_ref), (w_hbm, w_ref)), sems)
    cond_in.wait()
    cond = cond_ref[...].astype(jnp.float32)
    active = (cond / (1.0 + jnp.exp(-cond))).astype(jnp.bfloat16)
    active = jnp.broadcast_to(active, (16, active.shape[1]))
    copy.wait()
    piece = contract_last(active, w_ref[...])[0:1]
    out_ref[...] = jnp.broadcast_to(piece[None], out_ref.shape)


def prepare(
    lat_hbm,
    ctx_hbm,
    wk_hbm,
    wv_hbm,
    qg_ref,
    kg_ref,
    inv_ref,
    ctx_kv_ref,
    wkv_ref,
    gains_ref,
    lat_ref,
    ctx_ref,
    sems,
):
    rows = lat_ref.shape[0]
    head_dim = kg_ref.shape[1]
    copies = start_all(
        (
            (lat_hbm, lat_ref),
            (ctx_hbm, ctx_ref),
            (wk_hbm, wkv_ref.at[pl.ds(0, head_dim)]),
            (wv_hbm, wkv_ref.at[pl.ds(head_dim, head_dim)]),
        ),
        sems,
    )
    kg = jnp.concatenate([kg_ref[...]] * 2, axis=1)
    gains_ref[0:1, :] = jnp.concatenate([qg_ref[...]] * 2, axis=1)
    gains_ref[1:2, :] = kg
    copies[0].wait()
    step = 32
    for r in range(0, rows, step):
        x = lat_ref[r : r + step, :].astype(jnp.float32)
        mean_sq = jnp.mean(x * x, axis=-1, keepdims=True)
        inv_ref[r : r + step, :] = jnp.broadcast_to(lax.rsqrt(mean_sq + epsilon), (step, LANES))
    for copy in copies[1:]:
        copy.wait()
    scaled, _, low = turner(head_dim)
    both = contract_last(ctx_ref[...], wkv_ref[...])
    ctx_kv_ref[...] = jnp.where(low, scaled(both, kg), both).astype(jnp.bfloat16)


def project(
    lat_ref,
    wq_ref,
    wkv_ref,
    inv_ref,
    ctx_kv_ref,
    mod_ref,
    gain_ref,
    gains_ref,
    cos_ref,
    sin_ref,
    q_ref,
    main_hbm,
    rest_hbm,
    gate_ref,
    hid_ref,
    mods_ref,
    kv_ref,
    out_sems,
):
    rows, width = lat_ref.shape
    main = main_hbm.shape[0]
    rest = rest_hbm.shape[1]
    head_dim = wkv_ref.shape[0] // 2
    pieces, _, piece = mod_ref.shape
    for j in range(pieces):
        mods_ref[0:1, piece * j : piece * (j + 1)] = mod_ref[j]
    shift = mods_ref[0:1, 0:width]
    scale = 1.0 + mods_ref[0:1, width : 2 * width]
    gate_ref[...] = mods_ref[0:1, 2 * width : 3 * width]
    gain = gain_ref[...]
    step = 32
    for r in range(0, rows, step):
        x = lat_ref[r : r + step, :].astype(jnp.float32)
        hidden = x * inv_ref[r : r + step, 0:1] * gain * scale + shift
        hid_ref[r : r + step, :] = hidden.astype(jnp.bfloat16)

    scaled, turned, low = turner(head_dim)
    qg, kg = gains_ref[0:1, :], gains_ref[1:2, :]
    cosine, sine = cos_ref[...], sin_ref[...]
    hid = hid_ref[...]
    both = contract_last(hid, wkv_ref[...])
    both = jnp.where(low, turned(scaled(both, kg), cosine, sine), both).astype(jnp.bfloat16)
    kv_ref[0:rows, :] = both
    kv_ref[rows:, :] = ctx_kv_ref[...]
    sent = kv_ref.at[pl.ds(main, rest)]
    outs = start_all(
        [(kv_ref.at[pl.ds(0, main)], main_hbm)]
        + [(sent, rest_hbm.at[z]) for z in range(rest_hbm.shape[0])],
        out_sems,
    )
    queries = jnp.dot(hid, wq_ref[...], preferred_element_type=jnp.float32)
    for g in range(queries.shape[1] // LANES):
        pair = turned(scaled(queries[:, LANES * g : LANES * (g + 1)], qg), cosine, sine)
        pair = pair.astype(jnp.bfloat16).astype(jnp.float32) * head_dim**-0.5
        other = pltpu.roll(pair, head_dim, 1)
        q_ref[2 * g] = jnp.where(low, pair, 0.0).astype(jnp.bfloat16)
        q_ref[2 * g + 1] = jnp.where(low, other, 0.0).astype(jnp.bfloat16)
    for copy in outs:
        copy.wait()


def attend(q_ref, main_ref, rest_ref, w_hbm, o_ref, s_ref, at_ref, w_ref, sems):
    (weights_in,) = start_all(((w_hbm, w_ref),), sems)
    heads, rows, _ = q_ref.shape
    head_dim = at_ref.shape[1] // heads
    parts, at = [], 0
    for ref in (main_ref, rest_ref):
        count = ref.shape[0]
        for c in range(0, count, KEY_STEP):
            size = min(KEY_STEP, count - c)
            parts.append((ref, c, at, size))
            at += size
    row_max = None
    for h in range(heads + 1):
        if h < heads:
            q = q_ref[h]
            m = jnp.full((rows, LANES), -jnp.inf, jnp.float32)
        if h > 0:
            total = jnp.zeros((rows, LANES), jnp.float32)
            acc = jnp.zeros((rows, LANES), jnp.float32)
        for ref, c, at, size in parts:
            if h < heads:
                s = contract_last(q, ref[c : c + size, :])
                s_ref[h % 2, :, at : at + size] = s
                for j in range(0, size, LANES):
                    m = jnp.maximum(m, s[:, j : j + LANES])
            if h > 0:
                p = jnp.exp(s_ref[(h + 1) % 2, :, at : at + size] - row_max)
                for j in range(0, size, LANES):
                    total = total + p[:, j : j + LANES]
                acc = acc + jnp.dot(
                    p.astype(jnp.bfloat16), ref[c : c + size, :], preferred_element_type=jnp.float32
                )
        if h > 0:
            total = jnp.sum(total, axis=1, keepdims=True)
            at_ref[:, head_dim * (h - 1) : head_dim * h] = (acc[:, head_dim:] / total).astype(
                jnp.bfloat16
            )
        row_max = jnp.max(m, axis=1, keepdims=True)
    weights_in.wait()
    o_ref[...] = jnp.dot(at_ref[...], w_ref[...], preferred_element_type=jnp.float32).astype(
        jnp.bfloat16
    )


def finish(lat_ref, terms_ref, gate_ref, out_ref):
    kept = out_ref.shape[0]
    at = pl.multiple_of(lax.axis_index("tp") * kept, kept)
    projected = terms_ref[0].astype(jnp.float32)
    for g in range(1, terms_ref.shape[0]):
        projected = projected + terms_ref[g].astype(jnp.float32)
    residual = lat_ref[pl.ds(at, kept), :].astype(jnp.float32)
    out_ref[...] = (residual + gate_ref[...] * projected).astype(jnp.bfloat16)


def vmem(mebibytes):
    return pltpu.CompilerParams(vmem_limit_bytes=mebibytes * 2**20)


def in_vmem(count):
    return [pl.BlockSpec(memory_space=pltpu.VMEM)] * count


def in_hbm(count):
    return [pl.BlockSpec(memory_space=pltpu.HBM)] * count


def shards(
    latent,
    context,
    condition,
    mod_weight,
    norm_gain,
    w_query,
    w_key,
    w_value,
    q_gain,
    k_gain,
    w_out,
):
    _, length, width = latent.shape
    count = context.shape[1]
    head_dim = q_gain.shape[0]
    heads = w_query.shape[1] // head_dim
    sp, tp = lax.axis_size("sp"), lax.axis_size("tp")
    kept = length // tp
    main = length - 8
    rest = length - main + count
    half, single = jnp.bfloat16, jnp.float32
    shape = jax.ShapeDtypeStruct
    dma = lambda count: pltpu.SemaphoreType.DMA((count,))
    mod_pieces = pl.pallas_call(
        modulate,
        out_shape=shape((sp * tp, 1, mod_weight.shape[1]), single),
        in_specs=in_hbm(2),
        scratch_shapes=[
            pltpu.VMEM(condition.shape, half),
            pltpu.VMEM(mod_weight.shape[::-1], half),
            dma(2),
        ],
        compiler_params=vmem(60),
        name="modulate",
    )(condition, mod_weight.T)
    modulation = lax.all_to_all(mod_pieces, ("sp", "tp"), 0, 0, tiled=True)
    cosine, sine = rotary_tables(lax.axis_index("sp") * length, length, 0, head_dim)

    wk, wv = w_key.T, w_value.T
    inverse, ctx_kv, wkv, gains = pl.pallas_call(
        prepare,
        out_shape=(
            shape((length, LANES), single),
            shape((count, LANES), half),
            shape((2 * head_dim, width), half),
            shape((2, LANES), single),
        ),
        in_specs=in_hbm(4) + in_vmem(2),
        scratch_shapes=[pltpu.VMEM((length, width), half), pltpu.VMEM((count, width), half), dma(4)],
        compiler_params=vmem(52),
        name="prepare",
    )(latent[0], context[0], wk, wv, q_gain[None], k_gain[None])
    queries, own_main, own_rest, gate = pl.pallas_call(
        project,
        out_shape=(
            shape((heads, length, LANES), half),
            shape((main, LANES), half),
            shape((sp, rest, LANES), half),
            shape((1, width), single),
        ),
        in_specs=in_vmem(10),
        out_specs=tuple(in_vmem(1) + in_hbm(2) + in_vmem(1)),
        scratch_shapes=[
            pltpu.VMEM((length, width), half),
            pltpu.VMEM((8, 3 * width), single),
            pltpu.VMEM((main + rest, LANES), half),
            dma(1 + sp),
        ],
        compiler_params=vmem(16),
        name="project",
    )(
        latent[0],
        w_query,
        wkv,
        inverse,
        ctx_kv,
        modulation,
        norm_gain[None],
        gains,
        cosine,
        sine,
    )
    all_rest = lax.all_to_all(own_rest, "sp", 0, 0, tiled=True).reshape(sp * rest, LANES)
    all_main = lax.all_gather(own_main, "sp", axis=0, tiled=True)
    all_keys = sp * (main + rest)
    terms = pl.pallas_call(
        attend,
        out_shape=shape((length, width), half),
        in_specs=in_vmem(3) + in_hbm(1),
        scratch_shapes=[
            pltpu.VMEM((2, length, all_keys), single),
            pltpu.VMEM((length, heads * head_dim), half),
            pltpu.VMEM(w_out.shape, half),
            dma(1),
        ],
        compiler_params=vmem(32),
        name="attend",
    )(queries, all_main, all_rest, w_out)
    terms = lax.all_to_all(terms.reshape(tp, kept, width), "tp", 0, 0, tiled=True)
    mixed = pl.pallas_call(
        finish,
        out_shape=shape((kept, width), half),
        in_specs=in_vmem(3),
        compiler_params=vmem(8),
        name="finish",
    )(latent[0], terms, gate)
    return mixed[None]


def solution(mesh):
    placed = (
        P("dp", "sp", None),
        P("dp", "sp", None),
        P("dp", None),
        P(None, ("sp", "tp")),
        P(),
        P(None, "tp"),
        P(None, "tp"),
        P(None, "tp"),
        P(),
        P(),
        P("tp", None),
    )
    return jax.shard_map(
        shards, mesh=mesh, in_specs=placed, out_specs=P("dp", ("sp", "tp"), None), check_vma=False
    )
```

```python
import jax
import jax.numpy as jnp
from jax import lax
from jax.experimental import pallas as pl
from jax.experimental.pallas import tpu as pltpu
from jax.sharding import PartitionSpec as P

GRID_W = 64
LANES = 128
KEY_STEP = 512

epsilon = 1e-06
rope_base = 10000.0


def rotary_tables(first, rows, extra, head_dim):
    shape = (rows + extra, LANES)
    row = lax.broadcasted_iota(jnp.int32, shape, 0)
    lane = lax.broadcasted_iota(jnp.int32, shape, 1)
    where = first + row
    quarter = head_dim // 4
    place = jnp.where(lane % head_dim < head_dim // 2, where // GRID_W, where % GRID_W)
    place = jnp.where(row < rows, place, 0)
    freqs = rope_base ** (-(lane % quarter).astype(jnp.float32) / quarter)
    angle = place.astype(jnp.float32) * freqs
    sine = jnp.sin(angle)
    sine = jnp.where(lane % (2 * quarter) < quarter, -sine, sine)
    return jnp.where(lane < head_dim, jnp.cos(angle), sine)


def turner(head_dim):
    lane = lax.broadcasted_iota(jnp.int32, (1, LANES), 1)
    first = lane % (head_dim // 2) < head_dim // 4
    a = lax.broadcasted_iota(jnp.int32, (LANES, LANES), 0) // head_dim
    b = lax.broadcasted_iota(jnp.int32, (LANES, LANES), 1) // head_dim
    average = jnp.where(a == b, 1.0 / head_dim, 0.0).astype(jnp.float32)

    def scaled(values, gains):
        mean_sq = jnp.dot(
            values * values,
            average,
            preferred_element_type=jnp.float32,
            precision=lax.Precision.HIGHEST,
        )
        return values * lax.rsqrt(mean_sq + epsilon) * gains

    def turned(values, cosine, sine):
        ahead = pltpu.roll(values, LANES - head_dim // 4, 1)
        behind = pltpu.roll(values, head_dim // 4, 1)
        return values * cosine + jnp.where(first, ahead, behind) * sine

    return scaled, turned, lane < head_dim


def contract_last(a, b):
    return lax.dot_general(a, b, (((1,), (1,)), ((), ())), preferred_element_type=jnp.float32)


def start_all(pairs, sems):
    copies = [pltpu.make_async_copy(a, b, sems.at[i]) for i, (a, b) in enumerate(pairs)]
    for copy in copies:
        copy.start()
    return copies


def modulate(cond_hbm, w_hbm, out_ref, cond_ref, w_ref, sems):
    cond_in, copy = start_all(((cond_hbm, cond_ref), (w_hbm, w_ref)), sems)
    cond_in.wait()
    cond = cond_ref[...].astype(jnp.float32)
    active = (cond / (1.0 + jnp.exp(-cond))).astype(jnp.bfloat16)
    active = jnp.broadcast_to(active, (16, active.shape[1]))
    copy.wait()
    piece = contract_last(active, w_ref[...])[0:1]
    out_ref[...] = jnp.broadcast_to(piece[None], out_ref.shape)


def prepare(
    lat_hbm,
    ctx_hbm,
    wk_hbm,
    wv_hbm,
    qg_ref,
    kg_ref,
    inv_ref,
    ctx_kv_ref,
    wkv_ref,
    gains_ref,
    kept_ref,
    lat_ref,
    ctx_ref,
    sems,
):
    rows = lat_ref.shape[0]
    kept = kept_ref.shape[0]
    head_dim = kg_ref.shape[1]
    copies = start_all(
        (
            (lat_hbm, lat_ref),
            (ctx_hbm, ctx_ref),
            (wk_hbm, wkv_ref.at[pl.ds(0, head_dim)]),
            (wv_hbm, wkv_ref.at[pl.ds(head_dim, head_dim)]),
        ),
        sems,
    )
    kg = jnp.concatenate([kg_ref[...]] * 2, axis=1)
    gains_ref[0:1, :] = jnp.concatenate([qg_ref[...]] * 2, axis=1)
    gains_ref[1:2, :] = kg
    copies[0].wait()
    at = pl.multiple_of(lax.axis_index("tp") * kept, kept)
    kept_ref[...] = lat_ref[pl.ds(at, kept), :]
    step = 32
    for r in range(0, rows, step):
        x = lat_ref[r : r + step, :].astype(jnp.float32)
        mean_sq = jnp.mean(x * x, axis=-1, keepdims=True)
        inv_ref[r : r + step, :] = jnp.broadcast_to(lax.rsqrt(mean_sq + epsilon), (step, LANES))
    for copy in copies[1:]:
        copy.wait()
    scaled, _, low = turner(head_dim)
    both = contract_last(ctx_ref[...], wkv_ref[...])
    ctx_kv_ref[...] = jnp.where(low, scaled(both, kg), both).astype(jnp.bfloat16)


def project(
    lat_ref,
    wq_ref,
    wkv_ref,
    inv_ref,
    ctx_kv_ref,
    mod_ref,
    gain_ref,
    gains_ref,
    table_ref,
    q_ref,
    main_hbm,
    rest_hbm,
    gate_ref,
    hid_ref,
    mods_ref,
    kv_ref,
    out_sems,
):
    rows, width = lat_ref.shape
    main = main_hbm.shape[0]
    rest = rest_hbm.shape[1]
    head_dim = wkv_ref.shape[0] // 2
    pieces, _, piece = mod_ref.shape
    for j in range(pieces):
        mods_ref[0:1, piece * j : piece * (j + 1)] = mod_ref[j]
    shift = mods_ref[0:1, 0:width]
    scale = 1.0 + mods_ref[0:1, width : 2 * width]
    gate_ref[...] = mods_ref[0:1, 2 * width : 3 * width]
    gain = gain_ref[...]
    step = 32
    for r in range(0, rows, step):
        x = lat_ref[r : r + step, :].astype(jnp.float32)
        hidden = x * inv_ref[r : r + step, 0:1] * gain * scale + shift
        hid_ref[r : r + step, :] = hidden.astype(jnp.bfloat16)

    scaled, turned, low = turner(head_dim)
    qg, kg = gains_ref[0:1, :], gains_ref[1:2, :]
    table = table_ref[...]
    other = pltpu.roll(table, head_dim, 1)
    cosine, sine = jnp.where(low, table, other), jnp.where(low, other, table)
    hid = hid_ref[...]
    both = contract_last(hid, wkv_ref[...])
    both = jnp.where(low, turned(scaled(both, kg), cosine, sine), both).astype(jnp.bfloat16)
    kv_ref[0:rows, :] = both
    kv_ref[rows:, :] = ctx_kv_ref[...]
    sent = kv_ref.at[pl.ds(main, rest)]
    outs = start_all(
        [(kv_ref.at[pl.ds(0, main)], main_hbm)]
        + [(sent, rest_hbm.at[z]) for z in range(rest_hbm.shape[0])],
        out_sems,
    )
    queries = jnp.dot(hid, wq_ref[...], preferred_element_type=jnp.float32)
    for g in range(queries.shape[1] // LANES):
        pair = turned(scaled(queries[:, LANES * g : LANES * (g + 1)], qg), cosine, sine)
        pair = pair.astype(jnp.bfloat16).astype(jnp.float32) * head_dim**-0.5
        other = pltpu.roll(pair, head_dim, 1)
        q_ref[2 * g] = jnp.where(low, pair, 0.0).astype(jnp.bfloat16)
        q_ref[2 * g + 1] = jnp.where(low, other, 0.0).astype(jnp.bfloat16)
    for copy in outs:
        copy.wait()


def attend(q_ref, main_ref, rest_ref, w_hbm, o_ref, s_ref, at_ref, w_ref, sems):
    (weights_in,) = start_all(((w_hbm, w_ref),), sems)
    heads, rows, _ = q_ref.shape
    head_dim = at_ref.shape[1] // heads
    parts, at = [], 0
    for ref in (main_ref, rest_ref):
        count = ref.shape[0]
        for c in range(0, count, KEY_STEP):
            size = min(KEY_STEP, count - c)
            parts.append((ref, c, at, size))
            at += size
    row_max = None
    for h in range(heads + 1):
        if h < heads:
            q = q_ref[h]
            m = jnp.full((rows, LANES), -jnp.inf, jnp.float32)
        if h > 0:
            total = jnp.zeros((rows, LANES), jnp.float32)
            acc = jnp.zeros((rows, LANES), jnp.float32)
        for ref, c, at, size in parts:
            if h < heads:
                s = contract_last(q, ref[c : c + size, :])
                s_ref[h % 2, :, at : at + size] = s
                for j in range(0, size, LANES):
                    m = jnp.maximum(m, s[:, j : j + LANES])
            if h > 0:
                p = jnp.exp(s_ref[(h + 1) % 2, :, at : at + size] - row_max)
                for j in range(0, size, LANES):
                    total = total + p[:, j : j + LANES]
                acc = acc + jnp.dot(
                    p.astype(jnp.bfloat16), ref[c : c + size, :], preferred_element_type=jnp.float32
                )
        if h > 0:
            total = jnp.sum(total, axis=1, keepdims=True)
            at_ref[:, head_dim * (h - 1) : head_dim * h] = (acc[:, head_dim:] / total).astype(
                jnp.bfloat16
            )
        row_max = jnp.max(m, axis=1, keepdims=True)
    weights_in.wait()
    o_ref[...] = jnp.dot(at_ref[...], w_ref[...], preferred_element_type=jnp.float32).astype(
        jnp.bfloat16
    )


def finish(kept_ref, terms_ref, gate_ref, out_ref):
    projected = terms_ref[0].astype(jnp.float32)
    for g in range(1, terms_ref.shape[0]):
        projected = projected + terms_ref[g].astype(jnp.float32)
    residual = kept_ref[...].astype(jnp.float32)
    out_ref[...] = (residual + gate_ref[...] * projected).astype(jnp.bfloat16)


def vmem(mebibytes):
    return pltpu.CompilerParams(vmem_limit_bytes=mebibytes * 2**20)


def in_vmem(count):
    return [pl.BlockSpec(memory_space=pltpu.VMEM)] * count


def in_hbm(count):
    return [pl.BlockSpec(memory_space=pltpu.HBM)] * count


def shards(
    latent,
    context,
    condition,
    mod_weight,
    norm_gain,
    w_query,
    w_key,
    w_value,
    q_gain,
    k_gain,
    w_out,
):
    _, length, width = latent.shape
    count = context.shape[1]
    head_dim = q_gain.shape[0]
    heads = w_query.shape[1] // head_dim
    sp, tp = lax.axis_size("sp"), lax.axis_size("tp")
    kept = length // tp
    main = length - 8
    rest = length - main + count
    half, single = jnp.bfloat16, jnp.float32
    shape = jax.ShapeDtypeStruct
    dma = lambda count: pltpu.SemaphoreType.DMA((count,))
    mod_pieces = pl.pallas_call(
        modulate,
        out_shape=shape((sp * tp, 1, mod_weight.shape[1]), single),
        in_specs=in_hbm(2),
        scratch_shapes=[
            pltpu.VMEM(condition.shape, half),
            pltpu.VMEM(mod_weight.shape[::-1], half),
            dma(2),
        ],
        compiler_params=vmem(60),
        name="modulate",
    )(condition, mod_weight.T)
    modulation = lax.all_to_all(mod_pieces, ("sp", "tp"), 0, 0, tiled=True)
    table = rotary_tables(lax.axis_index("sp") * length, length, 0, head_dim)

    wk, wv = w_key.T, w_value.T
    inverse, ctx_kv, wkv, gains, kept_rows = pl.pallas_call(
        prepare,
        out_shape=(
            shape((length, LANES), single),
            shape((count, LANES), half),
            shape((2 * head_dim, width), half),
            shape((2, LANES), single),
            shape((kept, width), half),
        ),
        in_specs=in_hbm(4) + in_vmem(2),
        scratch_shapes=[pltpu.VMEM((length, width), half), pltpu.VMEM((count, width), half), dma(4)],
        compiler_params=vmem(52),
        name="prepare",
    )(latent[0], context[0], wk, wv, q_gain[None], k_gain[None])
    queries, own_main, own_rest, gate = pl.pallas_call(
        project,
        out_shape=(
            shape((heads, length, LANES), half),
            shape((main, LANES), half),
            shape((sp, rest, LANES), half),
            shape((1, width), single),
        ),
        in_specs=in_vmem(9),
        out_specs=tuple(in_vmem(1) + in_hbm(2) + in_vmem(1)),
        scratch_shapes=[
            pltpu.VMEM((length, width), half),
            pltpu.VMEM((8, 3 * width), single),
            pltpu.VMEM((main + rest, LANES), half),
            dma(1 + sp),
        ],
        compiler_params=vmem(16),
        name="project",
    )(
        latent[0],
        w_query,
        wkv,
        inverse,
        ctx_kv,
        modulation,
        norm_gain[None],
        gains,
        table,
    )
    all_rest = lax.all_to_all(own_rest, "sp", 0, 0, tiled=True).reshape(sp * rest, LANES)
    all_main = lax.all_gather(own_main, "sp", axis=0, tiled=True)
    all_keys = sp * (main + rest)
    terms = pl.pallas_call(
        attend,
        out_shape=shape((length, width), half),
        in_specs=in_vmem(3) + in_hbm(1),
        scratch_shapes=[
            pltpu.VMEM((2, length, all_keys), single),
            pltpu.VMEM((length, heads * head_dim), half),
            pltpu.VMEM(w_out.shape, half),
            dma(1),
        ],
        compiler_params=vmem(32),
        name="attend",
    )(queries, all_main, all_rest, w_out)
    terms = lax.all_to_all(terms.reshape(tp, kept, width), "tp", 0, 0, tiled=True)
    mixed = pl.pallas_call(
        finish,
        out_shape=shape((kept, width), half),
        in_specs=in_vmem(3),
        compiler_params=vmem(8),
        name="finish",
    )(kept_rows, terms, gate)
    return mixed[None]


def solution(mesh):
    placed = (
        P("dp", "sp", None),
        P("dp", "sp", None),
        P("dp", None),
        P(None, ("sp", "tp")),
        P(),
        P(None, "tp"),
        P(None, "tp"),
        P(None, "tp"),
        P(),
        P(),
        P("tp", None),
    )
    return jax.shard_map(
        shards, mesh=mesh, in_specs=placed, out_specs=P("dp", ("sp", "tp"), None), check_vma=False
    )
```

```python
import jax
import jax.numpy as jnp
from jax import lax
from jax.experimental import pallas as pl
from jax.experimental.pallas import tpu as pltpu
from jax.sharding import PartitionSpec as P

GRID_W = 64
LANES = 128
KEY_STEP = 512

epsilon = 1e-06
rope_base = 10000.0


def rotary_tables(first, rows, extra, head_dim):
    shape = (rows + extra, LANES)
    row = lax.broadcasted_iota(jnp.int32, shape, 0)
    lane = lax.broadcasted_iota(jnp.int32, shape, 1)
    where = first + row
    quarter = head_dim // 4
    place = jnp.where(lane % head_dim < head_dim // 2, where // GRID_W, where % GRID_W)
    place = jnp.where(row < rows, place, 0)
    freqs = rope_base ** (-(lane % quarter).astype(jnp.float32) / quarter)
    angle = place.astype(jnp.float32) * freqs
    sine = jnp.sin(angle)
    return jnp.cos(angle), jnp.where(lane % (2 * quarter) < quarter, -sine, sine)


def turner(head_dim):
    lane = lax.broadcasted_iota(jnp.int32, (1, LANES), 1)
    first = lane % (head_dim // 2) < head_dim // 4
    a = lax.broadcasted_iota(jnp.int32, (LANES, LANES), 0) // head_dim
    b = lax.broadcasted_iota(jnp.int32, (LANES, LANES), 1) // head_dim
    average = jnp.where(a == b, 1.0 / head_dim, 0.0).astype(jnp.float32)

    def scaled(values, gains):
        mean_sq = jnp.dot(
            values * values,
            average,
            preferred_element_type=jnp.float32,
            precision=lax.Precision.HIGHEST,
        )
        return values * lax.rsqrt(mean_sq + epsilon) * gains

    def turned(values, cosine, sine):
        ahead = pltpu.roll(values, LANES - head_dim // 4, 1)
        behind = pltpu.roll(values, head_dim // 4, 1)
        return values * cosine + jnp.where(first, ahead, behind) * sine

    return scaled, turned, lane < head_dim


def contract_last(a, b):
    return lax.dot_general(a, b, (((1,), (1,)), ((), ())), preferred_element_type=jnp.float32)


def start_all(pairs, sems):
    copies = [pltpu.make_async_copy(a, b, sems.at[i]) for i, (a, b) in enumerate(pairs)]
    for copy in copies:
        copy.start()
    return copies


def modulate(cond_hbm, w_hbm, out_ref, cond_ref, w_ref, sems):
    cond_in, copy = start_all(((cond_hbm, cond_ref), (w_hbm, w_ref)), sems)
    cond_in.wait()
    cond = cond_ref[...].astype(jnp.float32)
    active = (cond / (1.0 + jnp.exp(-cond))).astype(jnp.bfloat16)
    active = jnp.broadcast_to(active, (16, active.shape[1]))
    copy.wait()
    piece = contract_last(active, w_ref[...])[0:1]
    out_ref[...] = jnp.broadcast_to(piece[None], out_ref.shape)


def prepare(
    lat_hbm,
    ctx_hbm,
    wk_hbm,
    wv_hbm,
    qg_ref,
    kg_ref,
    inv_ref,
    ctx_kv_ref,
    wkv_ref,
    gains_ref,
    lat_ref,
    ctx_ref,
    sems,
):
    rows = lat_ref.shape[0]
    head_dim = kg_ref.shape[1]
    copies = start_all(
        (
            (lat_hbm, lat_ref),
            (ctx_hbm, ctx_ref),
            (wk_hbm, wkv_ref.at[pl.ds(0, head_dim)]),
            (wv_hbm, wkv_ref.at[pl.ds(head_dim, head_dim)]),
        ),
        sems,
    )
    kg = jnp.concatenate([kg_ref[...]] * 2, axis=1)
    gains_ref[0:1, :] = jnp.concatenate([qg_ref[...]] * 2, axis=1)
    gains_ref[1:2, :] = kg
    copies[0].wait()
    step = 32
    for r in range(0, rows, step):
        x = lat_ref[r : r + step, :].astype(jnp.float32)
        mean_sq = jnp.mean(x * x, axis=-1, keepdims=True)
        inv_ref[r : r + step, :] = jnp.broadcast_to(lax.rsqrt(mean_sq + epsilon), (step, LANES))
    for copy in copies[1:]:
        copy.wait()
    scaled, _, low = turner(head_dim)
    both = contract_last(ctx_ref[...], wkv_ref[...])
    ctx_kv_ref[...] = jnp.where(low, scaled(both, kg), both).astype(jnp.bfloat16)


def project(
    lat_ref,
    wq_ref,
    wkv_ref,
    inv_ref,
    ctx_kv_ref,
    mod_ref,
    gain_ref,
    gains_ref,
    cos_ref,
    sin_ref,
    q_ref,
    main_hbm,
    rest_hbm,
    gate_ref,
    hid_ref,
    mods_ref,
    kv_ref,
    out_sems,
):
    rows, width = lat_ref.shape
    main = main_hbm.shape[0]
    rest = rest_hbm.shape[1]
    head_dim = wkv_ref.shape[0] // 2
    pieces, _, piece = mod_ref.shape
    tp = lax.axis_size("tp")
    for j in range(pieces):
        at = piece * (j % (pieces // tp) * tp + j // (pieces // tp))
        mods_ref[0:1, at : at + piece] = mod_ref[j]
    shift = mods_ref[0:1, 0:width]
    scale = 1.0 + mods_ref[0:1, width : 2 * width]
    gate_ref[...] = mods_ref[0:1, 2 * width : 3 * width]
    gain = gain_ref[...]
    step = 32
    for r in range(0, rows, step):
        x = lat_ref[r : r + step, :].astype(jnp.float32)
        hidden = x * inv_ref[r : r + step, 0:1] * gain * scale + shift
        hid_ref[r : r + step, :] = hidden.astype(jnp.bfloat16)

    scaled, turned, low = turner(head_dim)
    qg, kg = gains_ref[0:1, :], gains_ref[1:2, :]
    cosine, sine = cos_ref[...], sin_ref[...]
    hid = hid_ref[...]
    both = contract_last(hid, wkv_ref[...])
    both = jnp.where(low, turned(scaled(both, kg), cosine, sine), both).astype(jnp.bfloat16)
    kv_ref[0:rows, :] = both
    kv_ref[rows:, :] = ctx_kv_ref[...]
    sent = kv_ref.at[pl.ds(main, rest)]
    outs = start_all(
        [(kv_ref.at[pl.ds(0, main)], main_hbm)]
        + [(sent, rest_hbm.at[z]) for z in range(rest_hbm.shape[0])],
        out_sems,
    )
    queries = jnp.dot(hid, wq_ref[...], preferred_element_type=jnp.float32)
    for g in range(queries.shape[1] // LANES):
        pair = turned(scaled(queries[:, LANES * g : LANES * (g + 1)], qg), cosine, sine)
        pair = pair.astype(jnp.bfloat16).astype(jnp.float32) * head_dim**-0.5
        other = pltpu.roll(pair, head_dim, 1)
        q_ref[2 * g] = jnp.where(low, pair, 0.0).astype(jnp.bfloat16)
        q_ref[2 * g + 1] = jnp.where(low, other, 0.0).astype(jnp.bfloat16)
    for copy in outs:
        copy.wait()


def attend(q_ref, main_ref, rest_ref, w_hbm, o_ref, s_ref, at_ref, w_ref, sems):
    (weights_in,) = start_all(((w_hbm, w_ref),), sems)
    heads, rows, _ = q_ref.shape
    head_dim = at_ref.shape[1] // heads
    parts, at = [], 0
    for ref in (main_ref, rest_ref):
        count = ref.shape[0]
        for c in range(0, count, KEY_STEP):
            size = min(KEY_STEP, count - c)
            parts.append((ref, c, at, size))
            at += size
    row_max = None
    for h in range(heads + 1):
        if h < heads:
            q = q_ref[h]
            m = jnp.full((rows, LANES), -jnp.inf, jnp.float32)
        if h > 0:
            total = jnp.zeros((rows, LANES), jnp.float32)
            acc = jnp.zeros((rows, LANES), jnp.float32)
        for ref, c, at, size in parts:
            if h < heads:
                s = contract_last(q, ref[c : c + size, :])
                s_ref[h % 2, :, at : at + size] = s
                for j in range(0, size, LANES):
                    m = jnp.maximum(m, s[:, j : j + LANES])
            if h > 0:
                p = jnp.exp(s_ref[(h + 1) % 2, :, at : at + size] - row_max)
                for j in range(0, size, LANES):
                    total = total + p[:, j : j + LANES]
                acc = acc + jnp.dot(
                    p.astype(jnp.bfloat16), ref[c : c + size, :], preferred_element_type=jnp.float32
                )
        if h > 0:
            total = jnp.sum(total, axis=1, keepdims=True)
            at_ref[:, head_dim * (h - 1) : head_dim * h] = (acc[:, head_dim:] / total).astype(
                jnp.bfloat16
            )
        row_max = jnp.max(m, axis=1, keepdims=True)
    weights_in.wait()
    o_ref[...] = jnp.dot(at_ref[...], w_ref[...], preferred_element_type=jnp.float32).astype(
        jnp.bfloat16
    )


def finish(lat_ref, terms_ref, gate_ref, out_ref):
    kept = out_ref.shape[0]
    at = pl.multiple_of(lax.axis_index("tp") * kept, kept)
    projected = terms_ref[0].astype(jnp.float32)
    for g in range(1, terms_ref.shape[0]):
        projected = projected + terms_ref[g].astype(jnp.float32)
    residual = lat_ref[pl.ds(at, kept), :].astype(jnp.float32)
    out_ref[...] = (residual + gate_ref[...] * projected).astype(jnp.bfloat16)


def vmem(mebibytes):
    return pltpu.CompilerParams(vmem_limit_bytes=mebibytes * 2**20)


def in_vmem(count):
    return [pl.BlockSpec(memory_space=pltpu.VMEM)] * count


def in_hbm(count):
    return [pl.BlockSpec(memory_space=pltpu.HBM)] * count


def shards(
    latent,
    context,
    condition,
    mod_weight,
    norm_gain,
    w_query,
    w_key,
    w_value,
    q_gain,
    k_gain,
    w_out,
):
    _, length, width = latent.shape
    count = context.shape[1]
    head_dim = q_gain.shape[0]
    heads = w_query.shape[1] // head_dim
    sp, tp = lax.axis_size("sp"), lax.axis_size("tp")
    kept = length // tp
    main = length - 8
    rest = length - main + count
    half, single = jnp.bfloat16, jnp.float32
    shape = jax.ShapeDtypeStruct
    dma = lambda count: pltpu.SemaphoreType.DMA((count,))
    mod_pieces = pl.pallas_call(
        modulate,
        out_shape=shape((sp * tp, 1, mod_weight.shape[1]), single),
        in_specs=in_hbm(2),
        scratch_shapes=[
            pltpu.VMEM(condition.shape, half),
            pltpu.VMEM(mod_weight.shape[::-1], half),
            dma(2),
        ],
        compiler_params=vmem(60),
        name="modulate",
    )(condition, mod_weight.T)
    modulation = lax.all_to_all(mod_pieces, ("tp", "sp"), 0, 0, tiled=True)
    cosine, sine = rotary_tables(lax.axis_index("sp") * length, length, 0, head_dim)

    wk, wv = w_key.T, w_value.T
    inverse, ctx_kv, wkv, gains = pl.pallas_call(
        prepare,
        out_shape=(
            shape((length, LANES), single),
            shape((count, LANES), half),
            shape((2 * head_dim, width), half),
            shape((2, LANES), single),
        ),
        in_specs=in_hbm(4) + in_vmem(2),
        scratch_shapes=[pltpu.VMEM((length, width), half), pltpu.VMEM((count, width), half), dma(4)],
        compiler_params=vmem(52),
        name="prepare",
    )(latent[0], context[0], wk, wv, q_gain[None], k_gain[None])
    queries, own_main, own_rest, gate = pl.pallas_call(
        project,
        out_shape=(
            shape((heads, length, LANES), half),
            shape((main, LANES), half),
            shape((sp, rest, LANES), half),
            shape((1, width), single),
        ),
        in_specs=in_vmem(10),
        out_specs=tuple(in_vmem(1) + in_hbm(2) + in_vmem(1)),
        scratch_shapes=[
            pltpu.VMEM((length, width), half),
            pltpu.VMEM((8, 3 * width), single),
            pltpu.VMEM((main + rest, LANES), half),
            dma(1 + sp),
        ],
        compiler_params=vmem(16),
        name="project",
    )(
        latent[0],
        w_query,
        wkv,
        inverse,
        ctx_kv,
        modulation,
        norm_gain[None],
        gains,
        cosine,
        sine,
    )
    all_rest = lax.all_to_all(own_rest, "sp", 0, 0, tiled=True).reshape(sp * rest, LANES)
    all_main = lax.all_gather(own_main, "sp", axis=0, tiled=True)
    all_keys = sp * (main + rest)
    terms = pl.pallas_call(
        attend,
        out_shape=shape((length, width), half),
        in_specs=in_vmem(3) + in_hbm(1),
        scratch_shapes=[
            pltpu.VMEM((2, length, all_keys), single),
            pltpu.VMEM((length, heads * head_dim), half),
            pltpu.VMEM(w_out.shape, half),
            dma(1),
        ],
        compiler_params=vmem(32),
        name="attend",
    )(queries, all_main, all_rest, w_out)
    terms = lax.all_to_all(terms.reshape(tp, kept, width), "tp", 0, 0, tiled=True)
    mixed = pl.pallas_call(
        finish,
        out_shape=shape((kept, width), half),
        in_specs=in_vmem(3),
        compiler_params=vmem(8),
        name="finish",
    )(latent[0], terms, gate)
    return mixed[None]


def solution(mesh):
    placed = (
        P("dp", "sp", None),
        P("dp", "sp", None),
        P("dp", None),
        P(None, ("sp", "tp")),
        P(),
        P(None, "tp"),
        P(None, "tp"),
        P(None, "tp"),
        P(),
        P(),
        P("tp", None),
    )
    return jax.shard_map(
        shards, mesh=mesh, in_specs=placed, out_specs=P("dp", ("sp", "tp"), None), check_vma=False
    )
```

```python
import jax
import jax.numpy as jnp
from jax import lax
from jax.experimental import pallas as pl
from jax.experimental.pallas import tpu as pltpu
from jax.sharding import PartitionSpec as P

GRID_W = 64
LANES = 128
KEY_STEP = 512

epsilon = 1e-06
rope_base = 10000.0


def rotary_tables(first, rows, extra, head_dim):
    shape = (rows + extra, LANES)
    row = lax.broadcasted_iota(jnp.int32, shape, 0)
    lane = lax.broadcasted_iota(jnp.int32, shape, 1)
    where = first + row
    quarter = head_dim // 4
    place = jnp.where(lane % head_dim < head_dim // 2, where // GRID_W, where % GRID_W)
    place = jnp.where(row < rows, place, 0)
    freqs = rope_base ** (-(lane % quarter).astype(jnp.float32) / quarter)
    angle = place.astype(jnp.float32) * freqs
    sine = jnp.sin(angle)
    return jnp.cos(angle), jnp.where(lane % (2 * quarter) < quarter, -sine, sine)


def turner(head_dim):
    lane = lax.broadcasted_iota(jnp.int32, (1, LANES), 1)
    first = lane % (head_dim // 2) < head_dim // 4
    a = lax.broadcasted_iota(jnp.int32, (LANES, LANES), 0) // head_dim
    b = lax.broadcasted_iota(jnp.int32, (LANES, LANES), 1) // head_dim
    average = jnp.where(a == b, 1.0 / head_dim, 0.0).astype(jnp.float32)

    def scaled(values, gains):
        mean_sq = jnp.dot(
            values * values,
            average,
            preferred_element_type=jnp.float32,
            precision=lax.Precision.HIGHEST,
        )
        return values * lax.rsqrt(mean_sq + epsilon) * gains

    def turned(values, cosine, sine):
        ahead = pltpu.roll(values, LANES - head_dim // 4, 1)
        behind = pltpu.roll(values, head_dim // 4, 1)
        return values * cosine + jnp.where(first, ahead, behind) * sine

    return scaled, turned, lane < head_dim


def contract_last(a, b):
    return lax.dot_general(a, b, (((1,), (1,)), ((), ())), preferred_element_type=jnp.float32)


def start_all(pairs, sems):
    copies = [pltpu.make_async_copy(a, b, sems.at[i]) for i, (a, b) in enumerate(pairs)]
    for copy in copies:
        copy.start()
    return copies


def modulate(cond_hbm, w_hbm, out_ref, cond_ref, w_ref, sems):
    rows = w_ref.shape[0] // 4
    cuts = [pl.ds(rows * k, rows) for k in range(4)]
    cond_in, *copies = start_all(
        [(cond_hbm, cond_ref)] + [(w_hbm.at[cut], w_ref.at[cut]) for cut in cuts], sems
    )
    cond_in.wait()
    cond = cond_ref[...].astype(jnp.float32)
    active = (cond / (1.0 + jnp.exp(-cond))).astype(jnp.bfloat16)
    active = jnp.broadcast_to(active, (16, active.shape[1]))
    for copy in copies:
        copy.wait()
    piece = contract_last(active, w_ref[...])[0:1]
    out_ref[...] = jnp.broadcast_to(piece[None], out_ref.shape)


def prepare(
    lat_hbm,
    ctx_hbm,
    wk_hbm,
    wv_hbm,
    qg_ref,
    kg_ref,
    inv_ref,
    ctx_kv_ref,
    wkv_ref,
    gains_ref,
    lat_ref,
    ctx_ref,
    sems,
):
    rows = lat_ref.shape[0]
    head_dim = kg_ref.shape[1]
    copies = start_all(
        (
            (lat_hbm, lat_ref),
            (ctx_hbm, ctx_ref),
            (wk_hbm, wkv_ref.at[pl.ds(0, head_dim)]),
            (wv_hbm, wkv_ref.at[pl.ds(head_dim, head_dim)]),
        ),
        sems,
    )
    kg = jnp.concatenate([kg_ref[...]] * 2, axis=1)
    gains_ref[0:1, :] = jnp.concatenate([qg_ref[...]] * 2, axis=1)
    gains_ref[1:2, :] = kg
    copies[0].wait()
    step = 32
    for r in range(0, rows, step):
        x = lat_ref[r : r + step, :].astype(jnp.float32)
        mean_sq = jnp.mean(x * x, axis=-1, keepdims=True)
        inv_ref[r : r + step, :] = jnp.broadcast_to(lax.rsqrt(mean_sq + epsilon), (step, LANES))
    for copy in copies[1:]:
        copy.wait()
    scaled, _, low = turner(head_dim)
    both = contract_last(ctx_ref[...], wkv_ref[...])
    ctx_kv_ref[...] = jnp.where(low, scaled(both, kg), both).astype(jnp.bfloat16)


def project(
    lat_ref,
    wq_ref,
    wkv_ref,
    inv_ref,
    ctx_kv_ref,
    mod_ref,
    gain_ref,
    gains_ref,
    cos_ref,
    sin_ref,
    q_ref,
    main_hbm,
    rest_hbm,
    gate_ref,
    hid_ref,
    mods_ref,
    kv_ref,
    out_sems,
):
    rows, width = lat_ref.shape
    main = main_hbm.shape[0]
    rest = rest_hbm.shape[1]
    head_dim = wkv_ref.shape[0] // 2
    pieces, _, piece = mod_ref.shape
    tp = lax.axis_size("tp")
    for j in range(pieces):
        at = piece * (j % (pieces // tp) * tp + j // (pieces // tp))
        mods_ref[0:1, at : at + piece] = mod_ref[j]
    shift = mods_ref[0:1, 0:width]
    scale = 1.0 + mods_ref[0:1, width : 2 * width]
    gate_ref[...] = mods_ref[0:1, 2 * width : 3 * width]
    gain = gain_ref[...]
    step = 32
    for r in range(0, rows, step):
        x = lat_ref[r : r + step, :].astype(jnp.float32)
        hidden = x * inv_ref[r : r + step, 0:1] * gain * scale + shift
        hid_ref[r : r + step, :] = hidden.astype(jnp.bfloat16)

    scaled, turned, low = turner(head_dim)
    qg, kg = gains_ref[0:1, :], gains_ref[1:2, :]
    cosine, sine = cos_ref[...], sin_ref[...]
    hid = hid_ref[...]
    both = contract_last(hid, wkv_ref[...])
    both = jnp.where(low, turned(scaled(both, kg), cosine, sine), both).astype(jnp.bfloat16)
    kv_ref[0:rows, :] = both
    kv_ref[rows:, :] = ctx_kv_ref[...]
    sent = kv_ref.at[pl.ds(main, rest)]
    outs = start_all(
        [(kv_ref.at[pl.ds(0, main)], main_hbm)]
        + [(sent, rest_hbm.at[z]) for z in range(rest_hbm.shape[0])],
        out_sems,
    )
    queries = jnp.dot(hid, wq_ref[...], preferred_element_type=jnp.float32)
    for g in range(queries.shape[1] // LANES):
        pair = turned(scaled(queries[:, LANES * g : LANES * (g + 1)], qg), cosine, sine)
        pair = pair.astype(jnp.bfloat16).astype(jnp.float32) * head_dim**-0.5
        other = pltpu.roll(pair, head_dim, 1)
        q_ref[2 * g] = jnp.where(low, pair, 0.0).astype(jnp.bfloat16)
        q_ref[2 * g + 1] = jnp.where(low, other, 0.0).astype(jnp.bfloat16)
    for copy in outs:
        copy.wait()


def attend(q_ref, main_ref, rest_ref, w_hbm, o_ref, s_ref, at_ref, w_ref, sems):
    (weights_in,) = start_all(((w_hbm, w_ref),), sems)
    heads, rows, _ = q_ref.shape
    head_dim = at_ref.shape[1] // heads
    parts, at = [], 0
    for ref in (main_ref, rest_ref):
        count = ref.shape[0]
        for c in range(0, count, KEY_STEP):
            size = min(KEY_STEP, count - c)
            parts.append((ref, c, at, size))
            at += size
    row_max = None
    for h in range(heads + 1):
        if h < heads:
            q = q_ref[h]
            m = jnp.full((rows, LANES), -jnp.inf, jnp.float32)
        if h > 0:
            total = jnp.zeros((rows, LANES), jnp.float32)
            acc = jnp.zeros((rows, LANES), jnp.float32)
        for ref, c, at, size in parts:
            if h < heads:
                s = contract_last(q, ref[c : c + size, :])
                s_ref[h % 2, :, at : at + size] = s
                for j in range(0, size, LANES):
                    m = jnp.maximum(m, s[:, j : j + LANES])
            if h > 0:
                p = jnp.exp(s_ref[(h + 1) % 2, :, at : at + size] - row_max)
                for j in range(0, size, LANES):
                    total = total + p[:, j : j + LANES]
                acc = acc + jnp.dot(
                    p.astype(jnp.bfloat16), ref[c : c + size, :], preferred_element_type=jnp.float32
                )
        if h > 0:
            total = jnp.sum(total, axis=1, keepdims=True)
            at_ref[:, head_dim * (h - 1) : head_dim * h] = (acc[:, head_dim:] / total).astype(
                jnp.bfloat16
            )
        row_max = jnp.max(m, axis=1, keepdims=True)
    weights_in.wait()
    o_ref[...] = jnp.dot(at_ref[...], w_ref[...], preferred_element_type=jnp.float32).astype(
        jnp.bfloat16
    )


def finish(lat_ref, terms_ref, gate_ref, out_ref):
    kept = out_ref.shape[0]
    at = pl.multiple_of(lax.axis_index("tp") * kept, kept)
    projected = terms_ref[0].astype(jnp.float32)
    for g in range(1, terms_ref.shape[0]):
        projected = projected + terms_ref[g].astype(jnp.float32)
    residual = lat_ref[pl.ds(at, kept), :].astype(jnp.float32)
    out_ref[...] = (residual + gate_ref[...] * projected).astype(jnp.bfloat16)


def vmem(mebibytes):
    return pltpu.CompilerParams(vmem_limit_bytes=mebibytes * 2**20)


def in_vmem(count):
    return [pl.BlockSpec(memory_space=pltpu.VMEM)] * count


def in_hbm(count):
    return [pl.BlockSpec(memory_space=pltpu.HBM)] * count


def shards(
    latent,
    context,
    condition,
    mod_weight,
    norm_gain,
    w_query,
    w_key,
    w_value,
    q_gain,
    k_gain,
    w_out,
):
    _, length, width = latent.shape
    count = context.shape[1]
    head_dim = q_gain.shape[0]
    heads = w_query.shape[1] // head_dim
    sp, tp = lax.axis_size("sp"), lax.axis_size("tp")
    kept = length // tp
    main = length - 8
    rest = length - main + count
    half, single = jnp.bfloat16, jnp.float32
    shape = jax.ShapeDtypeStruct
    dma = lambda count: pltpu.SemaphoreType.DMA((count,))
    mod_pieces = pl.pallas_call(
        modulate,
        out_shape=shape((sp * tp, 1, mod_weight.shape[1]), single),
        in_specs=in_hbm(2),
        scratch_shapes=[
            pltpu.VMEM(condition.shape, half),
            pltpu.VMEM(mod_weight.shape[::-1], half),
            dma(5),
        ],
        compiler_params=vmem(60),
        name="modulate",
    )(condition, mod_weight.T)
    modulation = lax.all_to_all(mod_pieces, ("tp", "sp"), 0, 0, tiled=True)
    cosine, sine = rotary_tables(lax.axis_index("sp") * length, length, 0, head_dim)

    wk, wv = w_key.T, w_value.T
    inverse, ctx_kv, wkv, gains = pl.pallas_call(
        prepare,
        out_shape=(
            shape((length, LANES), single),
            shape((count, LANES), half),
            shape((2 * head_dim, width), half),
            shape((2, LANES), single),
        ),
        in_specs=in_hbm(4) + in_vmem(2),
        scratch_shapes=[pltpu.VMEM((length, width), half), pltpu.VMEM((count, width), half), dma(4)],
        compiler_params=vmem(52),
        name="prepare",
    )(latent[0], context[0], wk, wv, q_gain[None], k_gain[None])
    queries, own_main, own_rest, gate = pl.pallas_call(
        project,
        out_shape=(
            shape((heads, length, LANES), half),
            shape((main, LANES), half),
            shape((sp, rest, LANES), half),
            shape((1, width), single),
        ),
        in_specs=in_vmem(10),
        out_specs=tuple(in_vmem(1) + in_hbm(2) + in_vmem(1)),
        scratch_shapes=[
            pltpu.VMEM((length, width), half),
            pltpu.VMEM((8, 3 * width), single),
            pltpu.VMEM((main + rest, LANES), half),
            dma(1 + sp),
        ],
        compiler_params=vmem(16),
        name="project",
    )(
        latent[0],
        w_query,
        wkv,
        inverse,
        ctx_kv,
        modulation,
        norm_gain[None],
        gains,
        cosine,
        sine,
    )
    all_rest = lax.all_to_all(own_rest, "sp", 0, 0, tiled=True).reshape(sp * rest, LANES)
    all_main = lax.all_gather(own_main, "sp", axis=0, tiled=True)
    all_keys = sp * (main + rest)
    terms = pl.pallas_call(
        attend,
        out_shape=shape((length, width), half),
        in_specs=in_vmem(3) + in_hbm(1),
        scratch_shapes=[
            pltpu.VMEM((2, length, all_keys), single),
            pltpu.VMEM((length, heads * head_dim), half),
            pltpu.VMEM(w_out.shape, half),
            dma(1),
        ],
        compiler_params=vmem(32),
        name="attend",
    )(queries, all_main, all_rest, w_out)
    terms = lax.all_to_all(terms.reshape(tp, kept, width), "tp", 0, 0, tiled=True)
    mixed = pl.pallas_call(
        finish,
        out_shape=shape((kept, width), half),
        in_specs=in_vmem(3),
        compiler_params=vmem(8),
        name="finish",
    )(latent[0], terms, gate)
    return mixed[None]


def solution(mesh):
    placed = (
        P("dp", "sp", None),
        P("dp", "sp", None),
        P("dp", None),
        P(None, ("sp", "tp")),
        P(),
        P(None, "tp"),
        P(None, "tp"),
        P(None, "tp"),
        P(),
        P(),
        P("tp", None),
    )
    return jax.shard_map(
        shards, mesh=mesh, in_specs=placed, out_specs=P("dp", ("sp", "tp"), None), check_vma=False
    )
```

```python
import jax
import jax.numpy as jnp
from jax import lax
from jax.experimental import pallas as pl
from jax.experimental.pallas import tpu as pltpu
from jax.sharding import PartitionSpec as P

GRID_W = 64
LANES = 128
KEY_STEP = 768

epsilon = 1e-06
rope_base = 10000.0


def rotary_tables(first, rows, extra, head_dim):
    shape = (rows + extra, LANES)
    row = lax.broadcasted_iota(jnp.int32, shape, 0)
    lane = lax.broadcasted_iota(jnp.int32, shape, 1)
    where = first + row
    quarter = head_dim // 4
    place = jnp.where(lane % head_dim < head_dim // 2, where // GRID_W, where % GRID_W)
    place = jnp.where(row < rows, place, 0)
    freqs = rope_base ** (-(lane % quarter).astype(jnp.float32) / quarter)
    angle = place.astype(jnp.float32) * freqs
    sine = jnp.sin(angle)
    return jnp.cos(angle), jnp.where(lane % (2 * quarter) < quarter, -sine, sine)


def turner(head_dim):
    lane = lax.broadcasted_iota(jnp.int32, (1, LANES), 1)
    first = lane % (head_dim // 2) < head_dim // 4
    a = lax.broadcasted_iota(jnp.int32, (LANES, LANES), 0) // head_dim
    b = lax.broadcasted_iota(jnp.int32, (LANES, LANES), 1) // head_dim
    average = jnp.where(a == b, 1.0 / head_dim, 0.0).astype(jnp.float32)

    def scaled(values, gains):
        mean_sq = jnp.dot(
            values * values,
            average,
            preferred_element_type=jnp.float32,
            precision=lax.Precision.HIGHEST,
        )
        return values * lax.rsqrt(mean_sq + epsilon) * gains

    def turned(values, cosine, sine):
        ahead = pltpu.roll(values, LANES - head_dim // 4, 1)
        behind = pltpu.roll(values, head_dim // 4, 1)
        return values * cosine + jnp.where(first, ahead, behind) * sine

    return scaled, turned, lane < head_dim


def contract_last(a, b):
    return lax.dot_general(a, b, (((1,), (1,)), ((), ())), preferred_element_type=jnp.float32)


def start_all(pairs, sems):
    copies = [pltpu.make_async_copy(a, b, sems.at[i]) for i, (a, b) in enumerate(pairs)]
    for copy in copies:
        copy.start()
    return copies


def modulate(cond_hbm, w_hbm, out_ref, cond_ref, w_ref, sems):
    cond_in, copy = start_all(((cond_hbm, cond_ref), (w_hbm, w_ref)), sems)
    cond_in.wait()
    cond = cond_ref[...].astype(jnp.float32)
    active = (cond / (1.0 + jnp.exp(-cond))).astype(jnp.bfloat16)
    active = jnp.broadcast_to(active, (16, active.shape[1]))
    copy.wait()
    piece = contract_last(active, w_ref[...])[0:1]
    out_ref[...] = jnp.broadcast_to(piece[None], out_ref.shape)


def prepare(
    lat_hbm,
    ctx_hbm,
    wk_hbm,
    wv_hbm,
    qg_ref,
    kg_ref,
    inv_ref,
    ctx_kv_ref,
    wkv_ref,
    gains_ref,
    lat_ref,
    ctx_ref,
    sems,
):
    rows = lat_ref.shape[0]
    head_dim = kg_ref.shape[1]
    copies = start_all(
        (
            (lat_hbm, lat_ref),
            (ctx_hbm, ctx_ref),
            (wk_hbm, wkv_ref.at[pl.ds(0, head_dim)]),
            (wv_hbm, wkv_ref.at[pl.ds(head_dim, head_dim)]),
        ),
        sems,
    )
    kg = jnp.concatenate([kg_ref[...]] * 2, axis=1)
    gains_ref[0:1, :] = jnp.concatenate([qg_ref[...]] * 2, axis=1)
    gains_ref[1:2, :] = kg
    copies[0].wait()
    step = 32
    for r in range(0, rows, step):
        x = lat_ref[r : r + step, :].astype(jnp.float32)
        mean_sq = jnp.mean(x * x, axis=-1, keepdims=True)
        inv_ref[r : r + step, :] = jnp.broadcast_to(lax.rsqrt(mean_sq + epsilon), (step, LANES))
    for copy in copies[1:]:
        copy.wait()
    scaled, _, low = turner(head_dim)
    both = contract_last(ctx_ref[...], wkv_ref[...])
    ctx_kv_ref[...] = jnp.where(low, scaled(both, kg), both).astype(jnp.bfloat16)


def project(
    lat_ref,
    wq_ref,
    wkv_ref,
    inv_ref,
    ctx_kv_ref,
    mod_ref,
    gain_ref,
    gains_ref,
    cos_ref,
    sin_ref,
    q_ref,
    main_hbm,
    rest_hbm,
    gate_ref,
    hid_ref,
    mods_ref,
    kv_ref,
    out_sems,
):
    rows, width = lat_ref.shape
    main = main_hbm.shape[0]
    rest = rest_hbm.shape[1]
    head_dim = wkv_ref.shape[0] // 2
    pieces, _, piece = mod_ref.shape
    tp = lax.axis_size("tp")
    for j in range(pieces):
        at = piece * (j % (pieces // tp) * tp + j // (pieces // tp))
        mods_ref[0:1, at : at + piece] = mod_ref[j]
    shift = mods_ref[0:1, 0:width]
    scale = 1.0 + mods_ref[0:1, width : 2 * width]
    gate_ref[...] = mods_ref[0:1, 2 * width : 3 * width]
    gain = gain_ref[...]
    step = 32
    for r in range(0, rows, step):
        x = lat_ref[r : r + step, :].astype(jnp.float32)
        hidden = x * inv_ref[r : r + step, 0:1] * gain * scale + shift
        hid_ref[r : r + step, :] = hidden.astype(jnp.bfloat16)

    scaled, turned, low = turner(head_dim)
    qg, kg = gains_ref[0:1, :], gains_ref[1:2, :]
    cosine, sine = cos_ref[...], sin_ref[...]
    hid = hid_ref[...]
    both = contract_last(hid, wkv_ref[...])
    both = jnp.where(low, turned(scaled(both, kg), cosine, sine), both).astype(jnp.bfloat16)
    kv_ref[0:rows, :] = both
    kv_ref[rows:, :] = ctx_kv_ref[...]
    sent = kv_ref.at[pl.ds(main, rest)]
    outs = start_all(
        [(kv_ref.at[pl.ds(0, main)], main_hbm)]
        + [(sent, rest_hbm.at[z]) for z in range(rest_hbm.shape[0])],
        out_sems,
    )
    queries = jnp.dot(hid, wq_ref[...], preferred_element_type=jnp.float32)
    for g in range(queries.shape[1] // LANES):
        pair = turned(scaled(queries[:, LANES * g : LANES * (g + 1)], qg), cosine, sine)
        pair = pair.astype(jnp.bfloat16).astype(jnp.float32) * head_dim**-0.5
        other = pltpu.roll(pair, head_dim, 1)
        q_ref[2 * g] = jnp.where(low, pair, 0.0).astype(jnp.bfloat16)
        q_ref[2 * g + 1] = jnp.where(low, other, 0.0).astype(jnp.bfloat16)
    for copy in outs:
        copy.wait()


def attend(q_ref, main_ref, rest_ref, w_hbm, o_ref, s_ref, at_ref, w_ref, sems):
    (weights_in,) = start_all(((w_hbm, w_ref),), sems)
    heads, rows, _ = q_ref.shape
    head_dim = at_ref.shape[1] // heads
    parts, at = [], 0
    for ref in (main_ref, rest_ref):
        count = ref.shape[0]
        for c in range(0, count, KEY_STEP):
            size = min(KEY_STEP, count - c)
            parts.append((ref, c, at, size))
            at += size
    row_max = None
    for h in range(heads + 1):
        if h < heads:
            q = q_ref[h]
            m = jnp.full((rows, LANES), -jnp.inf, jnp.float32)
        if h > 0:
            total = jnp.zeros((rows, LANES), jnp.float32)
            acc = jnp.zeros((rows, LANES), jnp.float32)
        for ref, c, at, size in parts:
            if h < heads:
                s = contract_last(q, ref[c : c + size, :])
                s_ref[h % 2, :, at : at + size] = s
                for j in range(0, size, LANES):
                    m = jnp.maximum(m, s[:, j : j + LANES])
            if h > 0:
                p = jnp.exp(s_ref[(h + 1) % 2, :, at : at + size] - row_max)
                for j in range(0, size, LANES):
                    total = total + p[:, j : j + LANES]
                acc = acc + jnp.dot(
                    p.astype(jnp.bfloat16), ref[c : c + size, :], preferred_element_type=jnp.float32
                )
        if h > 0:
            total = jnp.sum(total, axis=1, keepdims=True)
            at_ref[:, head_dim * (h - 1) : head_dim * h] = (acc[:, head_dim:] / total).astype(
                jnp.bfloat16
            )
        row_max = jnp.max(m, axis=1, keepdims=True)
    weights_in.wait()
    o_ref[...] = jnp.dot(at_ref[...], w_ref[...], preferred_element_type=jnp.float32).astype(
        jnp.bfloat16
    )


def finish(lat_ref, terms_ref, gate_ref, out_ref):
    kept = out_ref.shape[0]
    at = pl.multiple_of(lax.axis_index("tp") * kept, kept)
    projected = terms_ref[0].astype(jnp.float32)
    for g in range(1, terms_ref.shape[0]):
        projected = projected + terms_ref[g].astype(jnp.float32)
    residual = lat_ref[pl.ds(at, kept), :].astype(jnp.float32)
    out_ref[...] = (residual + gate_ref[...] * projected).astype(jnp.bfloat16)


def vmem(mebibytes):
    return pltpu.CompilerParams(vmem_limit_bytes=mebibytes * 2**20)


def in_vmem(count):
    return [pl.BlockSpec(memory_space=pltpu.VMEM)] * count


def in_hbm(count):
    return [pl.BlockSpec(memory_space=pltpu.HBM)] * count


def shards(
    latent,
    context,
    condition,
    mod_weight,
    norm_gain,
    w_query,
    w_key,
    w_value,
    q_gain,
    k_gain,
    w_out,
):
    _, length, width = latent.shape
    count = context.shape[1]
    head_dim = q_gain.shape[0]
    heads = w_query.shape[1] // head_dim
    sp, tp = lax.axis_size("sp"), lax.axis_size("tp")
    kept = length // tp
    main = length - 8
    rest = length - main + count
    half, single = jnp.bfloat16, jnp.float32
    shape = jax.ShapeDtypeStruct
    dma = lambda count: pltpu.SemaphoreType.DMA((count,))
    mod_pieces = pl.pallas_call(
        modulate,
        out_shape=shape((sp * tp, 1, mod_weight.shape[1]), single),
        in_specs=in_hbm(2),
        scratch_shapes=[
            pltpu.VMEM(condition.shape, half),
            pltpu.VMEM(mod_weight.shape[::-1], half),
            dma(2),
        ],
        compiler_params=vmem(60),
        name="modulate",
    )(condition, mod_weight.T)
    modulation = lax.all_to_all(mod_pieces, ("tp", "sp"), 0, 0, tiled=True)
    cosine, sine = rotary_tables(lax.axis_index("sp") * length, length, 0, head_dim)

    wk, wv = w_key.T, w_value.T
    inverse, ctx_kv, wkv, gains = pl.pallas_call(
        prepare,
        out_shape=(
            shape((length, LANES), single),
            shape((count, LANES), half),
            shape((2 * head_dim, width), half),
            shape((2, LANES), single),
        ),
        in_specs=in_hbm(4) + in_vmem(2),
        scratch_shapes=[pltpu.VMEM((length, width), half), pltpu.VMEM((count, width), half), dma(4)],
        compiler_params=vmem(52),
        name="prepare",
    )(latent[0], context[0], wk, wv, q_gain[None], k_gain[None])
    queries, own_main, own_rest, gate = pl.pallas_call(
        project,
        out_shape=(
            shape((heads, length, LANES), half),
            shape((main, LANES), half),
            shape((sp, rest, LANES), half),
            shape((1, width), single),
        ),
        in_specs=in_vmem(10),
        out_specs=tuple(in_vmem(1) + in_hbm(2) + in_vmem(1)),
        scratch_shapes=[
            pltpu.VMEM((length, width), half),
            pltpu.VMEM((8, 3 * width), single),
            pltpu.VMEM((main + rest, LANES), half),
            dma(1 + sp),
        ],
        compiler_params=vmem(16),
        name="project",
    )(
        latent[0],
        w_query,
        wkv,
        inverse,
        ctx_kv,
        modulation,
        norm_gain[None],
        gains,
        cosine,
        sine,
    )
    all_rest = lax.all_to_all(own_rest, "sp", 0, 0, tiled=True).reshape(sp * rest, LANES)
    all_main = lax.all_gather(own_main, "sp", axis=0, tiled=True)
    all_keys = sp * (main + rest)
    terms = pl.pallas_call(
        attend,
        out_shape=shape((length, width), half),
        in_specs=in_vmem(3) + in_hbm(1),
        scratch_shapes=[
            pltpu.VMEM((2, length, all_keys), single),
            pltpu.VMEM((length, heads * head_dim), half),
            pltpu.VMEM(w_out.shape, half),
            dma(1),
        ],
        compiler_params=vmem(32),
        name="attend",
    )(queries, all_main, all_rest, w_out)
    terms = lax.all_to_all(terms.reshape(tp, kept, width), "tp", 0, 0, tiled=True)
    mixed = pl.pallas_call(
        finish,
        out_shape=shape((kept, width), half),
        in_specs=in_vmem(3),
        compiler_params=vmem(8),
        name="finish",
    )(latent[0], terms, gate)
    return mixed[None]


def solution(mesh):
    placed = (
        P("dp", "sp", None),
        P("dp", "sp", None),
        P("dp", None),
        P(None, ("sp", "tp")),
        P(),
        P(None, "tp"),
        P(None, "tp"),
        P(None, "tp"),
        P(),
        P(),
        P("tp", None),
    )
    return jax.shard_map(
        shards, mesh=mesh, in_specs=placed, out_specs=P("dp", ("sp", "tp"), None), check_vma=False
    )
```
